32 devices in a mesh: rep: 2 (over x), fs: 8 (over z, y), tp: 2 (over core).
Axes of the slice: x: 2, y: 2, z: 4, core: 2. Of those that a mesh axis runs over, the one named last changes fastest.
Arguments:
- stream: bfloat16 [16, 1024, 2048], P(('rep', 'fs'), None, 'tp'), may hold values from -6 to 6
- norm_gain: float32 [2048], replicated, may hold values from 0.1 to 1.9
- w_in: float32 [2048, 512], P('fs', 'tp'), may hold values from -0.125 to 0.125
- s_in: float32 [512], P(('tp', 'fs')), may hold values from 0.1 to 1.9
- pool_w: bfloat16 [4, 128, 128], replicated, may hold values from -0.5 to 0.5
- w_out: float32 [512, 2048], P('fs', 'tp'), may hold values from -0.25 to 0.25
- s_out: float32 [2048], P(('tp', 'fs')), may hold values from 0.1 to 1.9
- ffn_gain: float32 [2048], replicated, may hold values from 0.1 to 1.9
- w_up: float32 [2048, 8192], P('fs', 'tp'), may hold values from -0.125 to 0.125
- s_up: float32 [8192], P(('tp', 'fs')), may hold values from 0.1 to 1.9
- w_down: float32 [8192, 2048], P('tp', 'fs'), may hold values from -0.0625 to 0.0625
- s_down: float32 [2048], P('fs'), may hold values from 0.1 to 1.9
Outputs:
- result: bfloat16 [16, 1024, 2048], P(('rep', 'fs'), None, 'tp')
The draws below stay inside these ranges and needn't reach their ends.
All inputs are finite; a program needn't handle non-finite values.
Results may differ from the reference program's by a relative error of at most 0.012.
Values may be sent and summed in bfloat16 or wider, within the bound.
A program may use at most 128 MiB of HBM per device.

```python
import jax
import jax.numpy as jnp
from jax import lax

D = 2048
FF = 8192
PW = 512
GROUP = 128
SEQ_LEN = 1024
BATCH = 16
N_TP = 2


def block_scale(stream_key, shape, cuts, least, top_value):
    level, own = 1.0, jax.random.fold_in(stream_key, 6)
    for axis_at, shards_of in cuts:
        draws = jnp.exp(jax.random.uniform(jax.random.fold_in(own, axis_at), (shards_of,), jnp.float32, least / len(cuts), top_value / len(cuts)))
        level = level * jnp.repeat(draws, shape[axis_at] // shards_of).reshape([-1 if axis == axis_at else 1 for axis in range(len(shape))])
    return level


def bell_draw(key, shape, scale, limit, shards=(), kind=jnp.bfloat16):
    entries = jax.random.normal(key, shape, jnp.float32) * scale
    if len(shards) > 0:
        entries = block_scale(key, shape, shards, -0.22, 0.18) * entries
    return jnp.clip(entries, min=-limit, max=limit).astype(kind)


def setup_inputs(seed: int = 0) -> dict:
    key_list = jax.random.split(jax.random.key(seed), 13)
    return {
        "stream": bell_draw(key_list[0], (BATCH, SEQ_LEN, D), 1.0, 6.0, ((0, 16), (2, 2))),
        "norm_gain": jnp.clip(1.0 + 0.18 * jax.random.normal(key_list[1], (D,), jnp.float32), 0.1, 1.9),
        "w_in": bell_draw(key_list[2], (D, PW), D ** -0.5, 0.125, ((0, 8), (1, 2)), jnp.float32),
        "s_in": jnp.clip(1.0 + 0.18 * jax.random.normal(key_list[3], (PW,), jnp.float32), 0.1, 1.9),
        "pool_w": bell_draw(key_list[4], (4, GROUP, GROUP), GROUP ** -0.5, 0.5),
        "w_out": bell_draw(key_list[5], (PW, D), PW ** -0.5, 0.25, ((0, 8), (1, 2)), jnp.float32),
        "s_out": jnp.clip(1.0 + 0.18 * jax.random.normal(key_list[6], (D,), jnp.float32), 0.1, 1.9),
        "ffn_gain": jnp.clip(1.0 + 0.18 * jax.random.normal(key_list[7], (D,), jnp.float32), 0.1, 1.9),
        "w_up": bell_draw(key_list[8], (D, FF), D ** -0.5, 0.125, ((0, 8), (1, 2)), jnp.float32),
        "s_up": jnp.clip(1.0 + 0.18 * jax.random.normal(key_list[9], (FF,), jnp.float32), 0.1, 1.9),
        "w_down": bell_draw(key_list[10], (FF, D), FF ** -0.5, 0.0625, ((0, 2), (1, 8)), jnp.float32),
        "s_down": jnp.clip(1.0 + 0.18 * jax.random.normal(key_list[11], (D,), jnp.float32), 0.1, 1.9),
    }


epsilon = 0.25

def rms_rows(values, gain):
    floats = values.astype(jnp.float32)
    scale = lax.rsqrt(lax.optimization_barrier(jnp.mean(floats * floats, axis=-1, keepdims=True)) + epsilon)
    return (floats * scale * gain).astype(jnp.bfloat16)

def pool_sequence(pool_in):
    length = pool_in.shape[0]
    floats = pool_in.astype(jnp.float32)
    running = jnp.concatenate([jnp.zeros((1, floats.shape[1]), jnp.float32), jnp.cumsum(floats, axis=0)], axis=0)
    positions = jnp.arange(length, dtype=jnp.int32)
    pieces = []
    for level in range(4):
        half = 2 ** level
        lower = jnp.clip(positions - half, 0, length).astype(jnp.int32)
        upper = jnp.clip(positions + half, 0, length).astype(jnp.int32)
        part = running[:, level * GROUP:(level + 1) * GROUP]
        counts = (upper - lower).astype(jnp.float32)[:, None]
        pieces.append((part[upper] - part[lower]) / counts - floats[:, level * GROUP:(level + 1) * GROUP])
    return jnp.concatenate(pieces, axis=1).astype(jnp.bfloat16)

def one_sequence(tokens, norm_gain, w_in, s_in, pool_w, w_out, s_out, ffn_gain, w_up, s_up, w_down, s_down):
    length = tokens.shape[0]
    normed = rms_rows(tokens, norm_gain)
    pool_in = (jnp.dot(normed, w_in.astype(jnp.bfloat16), preferred_element_type=jnp.float32) * s_in).astype(jnp.bfloat16)
    pooled = pool_sequence(pool_in)
    grouped = jnp.einsum('lgc,gcd->lgd', pooled.reshape(length, 4, GROUP).astype(jnp.float32), pool_w.astype(jnp.float32))
    grouped = grouped.reshape(length, PW).astype(jnp.bfloat16)
    branch = jnp.dot(grouped, w_out.astype(jnp.bfloat16), preferred_element_type=jnp.float32) * s_out
    mixed = (tokens.astype(jnp.float32) + branch).astype(jnp.bfloat16)
    ffn_in = rms_rows(mixed, ffn_gain)
    upward = jnp.dot(ffn_in, w_up.astype(jnp.bfloat16), preferred_element_type=jnp.float32) * s_up
    hidden = jnp.square(jax.nn.relu(upward)).astype(jnp.bfloat16)
    block = FF // N_TP
    hidden_blocks = hidden.reshape(length, N_TP, block).astype(jnp.float32)
    down_blocks = w_down.astype(jnp.bfloat16).reshape(N_TP, block, D).astype(jnp.float32)
    partials = jnp.einsum('ljf,jfd->jld', hidden_blocks, down_blocks) * s_down
    rounded = lax.optimization_barrier(partials.astype(jnp.bfloat16))
    summed = lax.optimization_barrier(jnp.sum(rounded.astype(jnp.float32), axis=0))
    return (mixed.astype(jnp.float32) + summed).astype(jnp.bfloat16)

def reference(stream, norm_gain, w_in, s_in, pool_w, w_out, s_out, ffn_gain, w_up, s_up, w_down, s_down):

    def single(tokens):
        return one_sequence(tokens, norm_gain, w_in, s_in, pool_w, w_out, s_out, ffn_gain, w_up, s_up, w_down, s_down)
    return lax.map(single, stream)
```

```python
import functools

import jax
import jax.numpy as jnp
from jax import lax
from jax.experimental import pallas as pl
from jax.experimental.pallas import tpu as pltpu
from jax.sharding import PartitionSpec as P

GROUP = 128


epsilon = 0.25
bf16 = jnp.bfloat16
f32 = jnp.float32


def dot(left, right):
    return jnp.dot(left, right, preferred_element_type=f32)


def rms_rows(values, gain):
    floats = values.astype(f32)
    scale = lax.rsqrt(jnp.mean(floats * floats, axis=-1, keepdims=True) + epsilon)
    return (floats * scale * gain).astype(bf16)


def shifted(value, axis_name, count, offset):
    return lax.ppermute(value, axis_name, [(i, (i + offset) % count) for i in range(count)])


def swap_gather(value, axis_name, count, axis):
    index = lax.axis_index(axis_name)
    width = value.shape[axis]
    shape = list(value.shape)
    shape[axis] = width * count
    if count == 2:
        other = shifted(value, axis_name, count, 1)
        low = jnp.where(index == 0, value, other)
        high = jnp.where(index == 0, other, value)
        return jnp.concatenate([low, high], axis=axis)
    full = jnp.zeros(shape, value.dtype)
    full = lax.dynamic_update_slice_in_dim(full, value, index * width, axis)
    for offset in range(1, count):
        piece = shifted(value, axis_name, count, offset)
        origin = (index - offset) % count
        full = lax.dynamic_update_slice_in_dim(full, piece, origin * width, axis)
    return full


def fs_sent(value, factors, offset_a, offset_b):
    n_a, n_b = factors
    pairs = []
    for i in range(n_a * n_b):
        pairs.append((i, ((i // n_b) ^ offset_a) * n_b + ((i % n_b) ^ offset_b)))
    return lax.ppermute(value, "fs", pairs)


def fs_pieces(value, factors):
    n_a, n_b = factors
    rows = [[value] for _ in range(n_a)]
    for x in range(1, n_a):
        rows[x] = [fs_sent(value, factors, x, 0)]
    for y in range(1, n_b):
        for x in range(n_a):
            rows[x].append(fs_sent(rows[x][0], factors, 0, y))
    return rows


def fs_origin(factors, x, y):
    index = lax.axis_index("fs")
    return ((index // factors[1]) ^ x) * factors[1] + ((index % factors[1]) ^ y)


def placed(rows, factors):
    block = rows[0][0].shape[0]
    width = rows[0][0].shape[1]
    full = jnp.zeros((block * factors[0] * factors[1], width), rows[0][0].dtype)
    for y in range(factors[1]):
        for x in range(factors[0]):
            full = lax.dynamic_update_slice_in_dim(
                full, rows[x][y], fs_origin(factors, x, y) * block, 0
            )
    return full


def pool_local(pool_in, first):
    length, width = pool_in.shape
    positions = jnp.arange(length, dtype=jnp.int32)
    source = positions[None, :]
    target = positions[:, None]
    group_of = (first + jnp.arange(width, dtype=jnp.int32)) // GROUP
    means = jnp.zeros((length, width), f32)
    for level in range(4):
        half = 2**level
        band_ones = ((source >= target - half) & (source < target + half)).astype(bf16)
        counts = (jnp.minimum(positions + half, length) - jnp.maximum(positions - half, 0)).astype(f32)
        sums = dot(band_ones, pool_in) / counts[:, None]
        means = jnp.where(group_of[None, :] == level, sums, means)
    return (means - pool_in.astype(f32)).astype(bf16)


def on_device(
    n_rep, n_fs, n_tp,
    stream, norm_gain, w_in, s_in, pool_w, w_out, s_out, ffn_gain, w_up, s_up, w_down, s_down,
):
    rep = lax.axis_index("rep")
    tokens = stream[0]
    length, local_width = tokens.shape
    hidden_width = w_up.shape[1] // n_rep

    n_a = n_tp * max(1, 4 // n_tp)
    factors = (n_a, n_fs // n_a)

    scales = jnp.concatenate([s_in, s_out, s_up, s_down])[None]
    scale_rows = [
        [scales if x == y == 0 else fs_sent(scales, factors, x, y) for y in range(factors[1])]
        for x in range(n_a)
    ]
    scales = placed(scale_rows, factors)
    ends, at = [], 0
    for part in (s_in, s_out, s_up, s_down):
        ends.append(scales[:, at:at + part.shape[0]])
        at += part.shape[0]
    scale_in, scale_out, scale_up = (part.reshape(-1) for part in ends[:3])
    scale_down = ends[3]

    in_rows = fs_pieces(w_in.astype(bf16), factors)
    out_rows = fs_pieces(w_out.astype(bf16), factors)
    w_in_all = placed(in_rows, factors)
    w_out_all = placed(out_rows, factors)

    up_own = lax.dynamic_slice_in_dim(w_up, rep * hidden_width, hidden_width, 1).astype(bf16)
    up_rows = fs_pieces(up_own, factors)
    up_all = placed(up_rows, factors)
    down_own = lax.dynamic_slice_in_dim(w_down, rep * hidden_width, hidden_width, 0).astype(bf16)
    down_own, *_ = lax.optimization_barrier((down_own, *[in_rows[x][0] for x in range(1, n_a)]))
    down_rows = fs_pieces(down_own, factors)

    normed = rms_rows(swap_gather(tokens, "tp", n_tp, 1), norm_gain)
    pool_in = (dot(normed, w_in_all) * scale_in).astype(bf16)
    pooled = pool_local(pool_in, lax.axis_index("tp") * pool_in.shape[1])
    pooled_all = swap_gather(pooled, "tp", n_tp, 1)
    groups = pool_w.shape[0]
    grouped = jnp.einsum(
        "lgc,gcd->lgd", pooled_all.reshape(length, groups, GROUP), pool_w, preferred_element_type=f32
    ).reshape(length, groups * GROUP).astype(bf16)
    mixed = (tokens.astype(f32) + dot(grouped, w_out_all) * scale_out).astype(bf16)

    mixed_own = swap_gather(mixed, "tp", n_tp, 1)
    sequences = [mixed_own]
    for offset in range(1, n_rep):
        other = shifted(mixed, "rep", n_rep, offset)
        sequences.append(swap_gather(other, "tp", n_tp, 1))
    scale_hidden = lax.dynamic_slice_in_dim(scale_up, rep * hidden_width, hidden_width, 0)
    hidden = []
    for rows in sequences:
        rows = rms_rows(rows, ffn_gain)
        upward = dot(rows, up_all)
        hidden.append(jnp.square(jax.nn.relu(upward * scale_hidden)).astype(bf16))

    hidden = jnp.concatenate(hidden, axis=0)
    width = w_down.shape[1]
    per_tp = n_a // n_tp
    tp = lax.axis_index("tp")
    turn = ((lax.axis_index("fs") // factors[1]) // per_tp) ^ tp
    result = jnp.zeros((length, local_width), bf16)
    for y in range(factors[1]):
        for xi in range(per_tp):
            stacked = jnp.stack([down_rows[xt * per_tp + xi][y] for xt in range(n_tp)])
            blocks, block_scales = [], []
            for k in range(n_tp):
                blocks.append(lax.dynamic_index_in_dim(stacked, turn ^ k, 0, keepdims=False))
                origin = fs_origin(factors, xi, y) ^ ((turn ^ k) * per_tp * factors[1])
                block_scales.append(lax.dynamic_index_in_dim(scale_down, origin, 0, keepdims=False))
            both = jnp.concatenate(blocks, axis=1)
            partial = (dot(hidden, both) * jnp.concatenate(block_scales)).astype(bf16)
            total = partial[:, :width].astype(f32)
            for k in range(1, n_tp):
                pairs = [(i, i ^ k) for i in range(n_tp)]
                total = total + lax.ppermute(partial[:, k * width:(k + 1) * width], "tp", pairs).astype(f32)
            own = total[:length]
            for k in range(1, n_rep):
                back = shifted(total[k * length:(k + 1) * length].astype(bf16), "rep", n_rep, -k)
                own = own + back.astype(f32)
            inner = (fs_origin(factors, xi, y) % (per_tp * factors[1])) * width
            mixed_part = lax.dynamic_slice_in_dim(mixed, inner, width, 1)
            piece = (mixed_part.astype(f32) + own).astype(bf16)
            result = lax.dynamic_update_slice_in_dim(result, piece, inner, 1)
    return result[None]


UP_TILE = (512, 512)
DOWN_ROWS = 512
MESH = pl.DeviceIdType.MESH
VMEM_BYTES = 67_043_328


def fused_kernel(
    n_fs, n_tp,
    stream, w_up, w_down, w_in, w_out, pool_w, norm_gain, ffn_gain, own_scales,
    out,
    up_all, down_all, up_other, down_other, ffn_rows, hidden, mixed, in_all, out_all,
    pool_in, grouped, squares, core_got, core_sent, pair_got, pair_sent, totals, pair_total,
    up_floats, scales, scale_in, scale_out, scale_up,
    load_sem, scale_send, scale_recv,
    mix_recv, mix_own_send, mix_z_send, mix_x_send, mix_y_send,
    piece_recv, own_send, z_send, x_send, y_send,
    core_send, core_recv, act_core_send, act_core_recv, act_pair_send, act_pair_recv,
    part_core_send, part_core_recv, part_pair_send, part_pair_recv, store_sem,
):
    rep, fs, tp = lax.axis_index("rep"), lax.axis_index("fs"), lax.axis_index("tp")
    n_z = n_fs // 2
    z, y = fs // 2, fs % 2
    length, local = stream.shape
    width = n_tp * local
    units = up_all.shape[1]
    block = down_all.shape[2]
    owned = n_fs // n_tp
    in_rows, out_rows = w_in.shape[0], w_out.shape[0]
    pool_width = pool_in.shape[1]
    core, across, pair = {"tp": 1 - tp}, {"rep": 1 - rep}, {"fs": fs + 1 - 2 * y}

    def remote(ref, there, sent, got, device):
        return pltpu.make_async_remote_copy(
            src_ref=ref, dst_ref=there, send_sem=sent, recv_sem=got,
            device_id=device, device_id_type=MESH,
        )

    def at_step(i):
        j, other = i // 2, i % 2
        both = jnp.minimum(z, n_z - 1 - z)
        paired = j <= 2 * both
        distance = jnp.where(paired, (j + 1) // 2, j - both)
        left = jnp.where(paired, j % 2 == 1, z > n_z - 1 - z)
        source = z + jnp.where(left, -distance, distance)
        return source * 2 + y + other - 2 * y * other, left

    def onward(left):
        return jnp.where(left, z < n_z - 1, z > 0), {"fs": fs + jnp.where(left, 2, -2)}

    def piece(kind, source, half):
        if kind == 0:
            rows = up_other.shape[0]
            return up_all.at[pl.ds(pl.multiple_of(source * rows + half * (rows // 2), rows // 2), rows // 2), :]
        return down_all.at[source, pl.ds(pl.multiple_of(half * (units // 2), units // 2), units // 2), :]

    def mix_piece(kind, source, half):
        ref, rows = ((in_all, in_rows), (out_all, out_rows))[kind]
        return ref.at[pl.ds(pl.multiple_of(source * rows + half * (rows // 2), rows // 2), rows // 2), :]

    def own_copy(kind, order, side):
        source = fs if order == 0 else fs + 1 - 2 * y
        ref = piece(kind, source, rep)
        return remote(ref, ref, own_send.at[kind, side, order], piece_recv.at[kind, source, rep],
                      {"fs": fs + (2 if side == 0 else -2)})

    def pair_copy(kind, half):
        if kind == 0:
            rows = up_other.shape[0] // 2
            ref = up_other.at[pl.ds(pl.multiple_of(half * rows, rows), rows), :]
        else:
            ref = down_other.at[pl.ds(pl.multiple_of(half * (units // 2), units // 2), units // 2), :]
        return remote(ref, piece(kind, fs, half), y_send.at[kind, half], piece_recv.at[kind, fs, half], pair)

    def onward_copy(kind, source, device):
        ref = piece(kind, source, rep)
        return remote(ref, ref, z_send.at[kind, source], piece_recv.at[kind, source, rep], device)

    def across_copy(kind, source):
        ref = piece(kind, source, rep)
        return remote(ref, ref, x_send.at[kind, source], piece_recv.at[kind, source, rep], across)

    def piece_wait(kind, source, half):
        ref = piece(kind, source, half)
        remote(ref, ref, x_send.at[kind, source], piece_recv.at[kind, source, half], across).wait_recv()

    def both_sides(act):
        @pl.when(z < n_z - 1)
        def _():
            act(0)

        @pl.when(z > 0)
        def _():
            act(1)

    def send_own(kind):
        both_sides(lambda side: own_copy(kind, 0, side).start())

    def send_pair(kind):
        for turn in range(2):
            pair_copy(kind, rep + turn - 2 * rep * turn).start()

    def pass_pair(kind):
        piece_wait(kind, fs + 1 - 2 * y, rep)
        both_sides(lambda side: own_copy(kind, 1, side).start())

    def pass_on(kind, i):
        source, left = at_step(i)
        piece_wait(kind, source, rep)
        going, device = onward(left)

        @pl.when(going)
        def _():
            onward_copy(kind, source, device).start()

        across_copy(kind, source).start()

    def mix_own_copy(kind, side):
        ref = mix_piece(kind, fs, rep)
        return remote(ref, ref, mix_own_send.at[kind, side], mix_recv.at[kind, fs, rep],
                      {"fs": fs + (2 if side == 0 else -2)})

    def mix_onward_copy(kind, source, device):
        ref = mix_piece(kind, source, rep)
        return remote(ref, ref, mix_z_send.at[kind, source], mix_recv.at[kind, source, rep], device)

    def mix_across_copy(kind, source):
        ref = mix_piece(kind, source, rep)
        return remote(ref, ref, mix_x_send.at[kind, source], mix_recv.at[kind, source, rep], across)

    def mix_pair_copy(kind, source, half):
        ref = mix_piece(kind, source, half)
        return remote(ref, ref, mix_y_send.at[kind, source, half], mix_recv.at[kind, source, half], pair)

    def mix_wait(kind, source, half):
        mix_pair_copy(kind, source, half).wait_recv()

    def scale_copy(offset):
        return remote(own_scales, scales.at[fs], scale_send.at[offset], scale_recv.at[fs],
                      {"fs": lax.rem(fs + offset, n_fs)})

    def core_copy(which, ref, there):
        return remote(ref, there, core_send.at[which], core_recv.at[which], core)

    my_half = pl.ds(pl.multiple_of(tp * local, local), local)
    my_pool = pl.ds(pl.multiple_of(tp * pool_width, pool_width), pool_width)
    n_tiles = 4
    tile = length // n_tiles

    def rows_of(t):
        return pl.ds(pl.multiple_of(t * tile, tile), tile)

    def act_pair_copy(t):
        return remote(ffn_rows.at[0, rows_of(t), my_half], ffn_rows.at[1, rows_of(t), my_half],
                      act_pair_send.at[t], act_pair_recv.at[t], pair)

    def act_core_copy(which, t):
        ref = ffn_rows.at[which, rows_of(t), my_half]
        return remote(ref, ref, act_core_send.at[which, t], act_core_recv.at[which, t], core)

    load_tokens = pltpu.make_async_copy(stream, mixed, load_sem.at[0])

    def load_up(which, half):
        return pltpu.make_async_copy(
            w_up.at[:, pl.ds(pl.multiple_of(half * units, units), units)], up_floats, load_sem.at[1 + which])

    quarter = units // 2

    def load_down(q):
        return pltpu.make_async_copy(
            w_down.at[pl.ds(q * quarter, quarter), :], totals.at[q], load_sem.at[3 + q])

    load_tokens.start()
    load_up(0, 1 - y).start()
    for q in range(4):
        load_down(q).start()

    own_in = pl.ds(pl.multiple_of(fs * in_rows, in_rows), in_rows)
    own_out = pl.ds(pl.multiple_of(fs * out_rows, out_rows), out_rows)
    in_all[own_in, :] = w_in[...].astype(bf16)
    out_all[own_out, :] = w_out[...].astype(bf16)

    barrier = pltpu.get_barrier_semaphore()
    for offset in range(1, n_fs):
        pl.semaphore_signal(barrier, inc=1, device_id={"fs": lax.rem(fs + offset, n_fs)}, device_id_type=MESH)
    pl.semaphore_signal(barrier, inc=1, device_id=across, device_id_type=MESH)
    pl.semaphore_signal(barrier, inc=1, device_id=core, device_id_type=MESH)
    pl.semaphore_wait(barrier, n_fs + 1)

    for kind in range(2):
        both_sides(lambda side, kind=kind: mix_own_copy(kind, side).start())
        for half in range(2):
            mix_pair_copy(kind, fs, half).start()
    for offset in range(1, n_fs):
        scale_copy(offset).start()
    scales[fs] = own_scales[...]

    load_tokens.wait()

    def square_rows(t, carry):
        floats = mixed[rows_of(t), :].astype(f32)
        total = jnp.sum(floats * floats, axis=1, keepdims=True)
        squares[0, rows_of(t), :] = jnp.broadcast_to(total, (tile, 128))
        return carry

    lax.fori_loop(0, n_tiles, square_rows, 0)
    share_squares = core_copy(0, squares.at[0], squares.at[1])
    share_squares.start()

    def mix_step(j):
        source, left = at_step(2 * j)
        going, device = onward(left)
        for kind in range(2):
            mix_wait(kind, source, rep)

            @pl.when(going)
            def _():
                mix_onward_copy(kind, source, device).start()

            mix_across_copy(kind, source).start()
            mix_pair_copy(kind, source, rep).start()

    load_up(0, 1 - y).wait()
    pieces = 8
    up_tile = up_floats.shape[0] // pieces

    def cast_other(t, carry):
        rows = pl.ds(pl.multiple_of(t * up_tile, up_tile), up_tile)
        up_other[rows, :] = up_floats[rows, :].astype(bf16)
        return carry

    lax.fori_loop(0, pieces, cast_other, 0)
    load_up(1, y).start()

    share_squares.wait()

    def normed_rows(t, carry):
        rows = rows_of(t)
        total = squares[0, rows, :] + squares[1, rows, :]
        scale = lax.rsqrt(total[:, :1] * (1.0 / width) + epsilon)
        floats = mixed[rows, :].astype(f32)
        hidden[1, rows, my_half] = (floats * scale * norm_gain[pl.ds(tp, 1), :]).astype(bf16)
        return carry

    lax.fori_loop(0, n_tiles, normed_rows, 0)
    share_normed = core_copy(1, hidden.at[1, :, my_half], hidden.at[1, :, my_half])
    share_normed.start()

    mix_step(1)

    load_up(1, y).wait()

    def cast_own(t, carry):
        rows = pl.ds(pl.multiple_of(t * up_tile, up_tile), up_tile)
        there = pl.ds(pl.multiple_of(fs * up_floats.shape[0] + t * up_tile, up_tile), up_tile)
        up_all[there, :] = up_floats[rows, :].astype(bf16)
        return carry

    lax.fori_loop(0, pieces, cast_own, 0)

    for j in range(2, n_z):
        mix_step(j)
    send_own(0)
    send_pair(0)

    for q in range(4):
        load_down(q).wait()
    down_tile = quarter // pieces

    def cast_down(t, carry):
        rows = pl.ds(pl.multiple_of(t * down_tile, down_tile), down_tile)
        for half in range(2):
            there = pl.ds(pl.multiple_of(half * quarter + t * down_tile, down_tile), down_tile)
            down_all[fs, there, :] = totals[2 * y + half, rows, :].astype(bf16)
            down_other[there, :] = totals[2 - 2 * y + half, rows, :].astype(bf16)
        return carry

    lax.fori_loop(0, pieces, cast_down, 0)

    for j in range(1, n_z):
        source, _ = at_step(2 * j)
        for kind in range(2):
            mix_wait(kind, source, 1 - rep)
            mix_pair_copy(kind, source, 1 - rep).start()
    send_own(1)

    for offset in range(1, n_fs):
        source = lax.rem(fs + offset, n_fs)
        remote(own_scales, scales.at[source], scale_send.at[offset], scale_recv.at[source], pair).wait_recv()
    gathered = scales[...]
    summed = jnp.sum(gathered[:, 0:2, :], axis=0)
    scale_in[...] = jnp.concatenate([summed[0:1], summed[1:2]], axis=1)
    for source in range(n_fs):
        scale_out[:, source * 128:(source + 1) * 128] = gathered[source, 2:3, :]
    per = units // (n_fs // 2)
    for q in range(n_fs // 2):
        rows = scales[y * (n_fs // 2) + q]
        for i in range(per // 128):
            scale_up[:, q * per + i * 128:q * per + (i + 1) * 128] = rows[3 + i:4 + i, :]

    for source_z in range(n_z):
        for kind in range(2):
            for half in range(2):
                mix_wait(kind, source_z * 2 + 1 - y, half)

    share_normed.wait()

    def pool_rows(t, carry):
        rows = rows_of(t)
        product = jnp.dot(hidden[1, rows, :], in_all[...], preferred_element_type=f32)
        pool_in[rows, :] = (product * scale_in[...]).astype(bf16)
        return carry

    lax.fori_loop(0, n_tiles, pool_rows, 0)
    pass_pair(0)
    per_core = pool_width // GROUP

    def group_rows(t, carry):
        rows = rows_of(t)
        target = lax.broadcasted_iota(jnp.int32, (tile, length), 0) + t * tile
        source = lax.broadcasted_iota(jnp.int32, (tile, length), 1)
        gap = source - target
        at = lax.broadcasted_iota(jnp.int32, (tile, GROUP), 0) + t * tile
        for g in range(per_core):
            half = jnp.left_shift(jnp.int32(1), tp * per_core + g)
            lanes = slice(g * GROUP, (g + 1) * GROUP)
            band = jnp.where((gap >= -half) & (gap < half), 1.0, 0.0).astype(bf16)
            sums = jnp.dot(band, pool_in[:, lanes], preferred_element_type=f32)
            counts = (jnp.minimum(at + half, length) - jnp.maximum(at - half, 0)).astype(f32)
            pooled = (sums / counts - pool_in[rows, lanes].astype(f32)).astype(bf16)
            product = jnp.dot(pooled, pool_w[tp * per_core + g], preferred_element_type=f32)
            there = pl.ds(pl.multiple_of(tp * pool_width + g * GROUP, GROUP), GROUP)
            grouped[rows, there] = product.astype(bf16)
        return carry

    lax.fori_loop(0, n_tiles, group_rows, 0)
    share_grouped = core_copy(2, grouped.at[:, my_pool], grouped.at[:, my_pool])
    share_grouped.start()
    pass_on(0, 2)
    share_grouped.wait()

    def mix_rows(t, carry):
        rows = rows_of(t)
        product = jnp.dot(grouped[rows, :], out_all[...], preferred_element_type=f32)
        total = (mixed[rows, :].astype(f32) + product * scale_out[...]).astype(bf16)
        mixed[rows, :] = total
        floats = total.astype(f32)
        squares[0, rows, :] = jnp.broadcast_to(jnp.sum(floats * floats, axis=1, keepdims=True), (tile, 128))
        return carry

    lax.fori_loop(0, n_tiles, mix_rows, 0)
    share_more = core_copy(3, squares.at[0], squares.at[1])
    share_more.start()
    share_more.wait()

    def ffn_in_rows(t, carry):
        rows = rows_of(t)
        total = squares[0, rows, :] + squares[1, rows, :]
        scale = lax.rsqrt(total[:, :1] * (1.0 / width) + epsilon)
        floats = mixed[rows, :].astype(f32)
        ffn_rows[0, rows, my_half] = (floats * scale * ffn_gain[pl.ds(tp, 1), :]).astype(bf16)
        act_pair_copy(t).start()
        act_core_copy(0, t).start()
        return carry

    lax.fori_loop(0, n_tiles, ffn_in_rows, 0)
    send_pair(1)

    for i in range(3, 2 * n_z):
        pass_on(0, i)
    piece_wait(0, fs + 1 - 2 * y, 1 - rep)

    def up_ready(i, carry):
        source, _ = at_step(i)
        piece_wait(0, source, 1 - rep)
        return carry

    lax.fori_loop(2, 2 * n_z, up_ready, 0)
    for t in range(n_tiles):
        act_core_copy(0, t).wait_recv()

    up_rows, up_columns = UP_TILE
    n_rows, n_columns = length // up_rows, units // up_columns

    def up_tiles(sequence):
        def body(n, carry):
            rows = pl.ds(pl.multiple_of((n % n_rows) * up_rows, up_rows), up_rows)
            columns = pl.ds(pl.multiple_of((n // n_rows) * up_columns, up_columns), up_columns)
            product = jnp.dot(ffn_rows[sequence, rows, :], up_all[:, columns], preferred_element_type=f32)
            positive = jnp.maximum(product * scale_up[:, columns], 0.0)
            hidden[sequence, rows, columns] = (positive * positive).astype(bf16)
            return carry

        return body

    pass_pair(1)
    lax.fori_loop(0, n_rows * n_columns, up_tiles(0), 0)
    for t in range(n_tiles):
        act_pair_copy(t).wait_recv()
        act_core_copy(1, t).start()
    pass_on(1, 2)
    for t in range(n_tiles):
        act_core_copy(1, t).wait_recv()
    lax.fori_loop(0, n_rows * n_columns // 2, up_tiles(1), 0)
    pass_on(1, 3)
    lax.fori_loop(n_rows * n_columns // 2, n_rows * n_columns, up_tiles(1), 0)

    down_rows = DOWN_ROWS

    def part_core_copy(index, sequence):
        span = pl.ds(sequence * length, length)
        return remote(core_sent.at[index, span, :], core_got.at[index, span, :],
                      part_core_send.at[index, sequence], part_core_recv.at[index, sequence], core)

    def part_pair_copy(index):
        return remote(pair_sent.at[index], pair_got.at[index],
                      part_pair_send.at[index], part_pair_recv.at[index], pair)

    def down_block(i, carry):
        @pl.when((i >= 3) & (i < 2 * n_z - 1))
        def _():
            pass_on(1, i + 1)

        source, _ = at_step(i)

        @pl.when(i > 0)
        def _():
            piece_wait(1, source, 1 - rep)

        index = source % owned
        mine = source // owned == tp
        scale = jnp.concatenate([scales[source, 7:8, :], scales[source, 8:9, :]], axis=1)
        for sequence in (1, 0):
            def down_tile_rows(m, inner):
                rows = pl.ds(pl.multiple_of(m * down_rows, down_rows), down_rows)
                product = jnp.dot(hidden[sequence, rows, :], down_all[source], preferred_element_type=f32) * scale

                @pl.when(mine)
                def _():
                    if sequence == 1:
                        pair_total[rows, :] = product
                    else:
                        totals[index, rows, :] = product

                @pl.when(jnp.logical_not(mine))
                def _():
                    there = pl.ds(pl.multiple_of(sequence * length + m * down_rows, down_rows), down_rows)
                    core_sent[index, there, :] = product.astype(bf16)

                return inner

            lax.fori_loop(0, length // down_rows, down_tile_rows, 0)

            @pl.when(jnp.logical_not(mine))
            def _():
                part_core_copy(index, sequence).start()

        @pl.when(mine)
        def _():
            part_core_copy(index, 1).wait_recv()
            pair_sent[index] = (pair_total[...] + core_got[index, length:2 * length, :].astype(f32)).astype(bf16)
            part_pair_copy(index).start()

        return carry

    lax.fori_loop(0, n_fs, down_block, 0)

    def store_block(index):
        columns = pl.ds(pl.multiple_of(index * block, block), block)
        return pltpu.make_async_copy(pair_sent.at[index], out.at[:, columns], store_sem.at[index])

    def finish_block(i, carry):
        source, _ = at_step(i)

        @pl.when(source // owned == tp)
        def _():
            index = source % owned
            columns = pl.ds(pl.multiple_of(index * block, block), block)
            part_core_copy(index, 0).wait_recv()
            part_pair_copy(index).wait()
            total = totals[index] + core_got[index, 0:length, :].astype(f32) + pair_got[index].astype(f32)
            pair_sent[index] = (mixed[:, columns].astype(f32) + total).astype(bf16)
            store_block(index).start()

        return carry

    lax.fori_loop(0, n_fs, finish_block, 0)

    for kind in range(2):
        both_sides(lambda side, kind=kind: mix_own_copy(kind, side).wait_send())
        for order in range(2):
            both_sides(lambda side, kind=kind, order=order: own_copy(kind, order, side).wait_send())
        for half in range(2):
            mix_pair_copy(kind, fs, half).wait_send()
            pair_copy(kind, half).wait_send()

        def sent_step(i, carry, kind=kind):
            source, left = at_step(i)
            going, device = onward(left)

            @pl.when(going)
            def _():
                onward_copy(kind, source, device).wait_send()

            across_copy(kind, source).wait_send()

            @pl.when(i % 2 == 0)
            def _():
                @pl.when(going)
                def _():
                    mix_onward_copy(kind, source, device).wait_send()

                mix_across_copy(kind, source).wait_send()
                mix_pair_copy(kind, source, 0).wait_send()
                mix_pair_copy(kind, source, 1).wait_send()

            return carry

        lax.fori_loop(2, 2 * n_z, sent_step, 0)
    for offset in range(1, n_fs):
        scale_copy(offset).wait_send()
    for t in range(n_tiles):
        act_pair_copy(t).wait_send()
        for which in range(2):
            act_core_copy(which, t).wait_send()
    for index in range(owned):
        for sequence in range(2):
            part_core_copy(index, sequence).wait_send()
        store_block(index).wait()


def fused(n_fs, n_tp, stream, norm_gain, w_in, s_in, pool_w, w_out, s_out,
          ffn_gain, w_up, s_up, w_down, s_down):
    fs = lax.axis_index("fs")
    tokens = stream[0]
    length, local = tokens.shape
    rows, all_units = w_up.shape
    units = all_units // 2
    block = w_down.shape[1]
    in_rows, pool_width = w_in.shape
    out_rows = w_out.shape[0]
    owned = n_fs // n_tp
    placed_in = lax.dynamic_update_slice(jnp.zeros((pool_width,), f32), s_in, (fs * s_in.shape[0],))
    packed = jnp.concatenate([placed_in, s_out, s_up, s_down])
    packed = jnp.pad(packed, (0, 16 * 128 - packed.shape[0])).reshape(16, 128)
    vmem, anywhere = pl.BlockSpec(memory_space=pltpu.VMEM), pl.BlockSpec(memory_space=pl.ANY)
    dma = pltpu.SemaphoreType.DMA
    result = pl.pallas_call(
        functools.partial(fused_kernel, n_fs, n_tp),
        out_shape=jax.ShapeDtypeStruct((length, local), bf16),
        in_specs=[anywhere] * 3 + [vmem] * 6,
        out_specs=anywhere,
        scratch_shapes=[
            pltpu.VMEM((rows * n_fs, units), bf16),
            pltpu.VMEM((n_fs, units, block), bf16),
            pltpu.VMEM((rows, units), bf16),
            pltpu.VMEM((units, block), bf16),
            pltpu.VMEM((2, length, n_tp * local), bf16),
            pltpu.VMEM((2, length, units), bf16),
            pltpu.VMEM((length, local), bf16),
            pltpu.VMEM((in_rows * n_fs, pool_width), bf16),
            pltpu.VMEM((out_rows * n_fs, local), bf16),
            pltpu.VMEM((length, pool_width), bf16),
            pltpu.VMEM((length, n_tp * pool_width), bf16),
            pltpu.VMEM((2, length, 128), f32),
            pltpu.VMEM((owned, 2 * length, block), bf16),
            pltpu.VMEM((owned, 2 * length, block), bf16),
            pltpu.VMEM((owned, length, block), bf16),
            pltpu.VMEM((owned, length, block), bf16),
            pltpu.VMEM((owned, length, block), f32),
            pltpu.VMEM((length, block), f32),
            pltpu.VMEM((rows, units), f32),
            pltpu.VMEM((n_fs, 16, 128), f32),
            pltpu.VMEM((1, pool_width), f32),
            pltpu.VMEM((1, local), f32),
            pltpu.VMEM((1, units), f32),
            dma((7,)), dma((n_fs,)), dma((n_fs,)),
            dma((2, n_fs, 2)), dma((2, 2)), dma((2, n_fs)), dma((2, n_fs)), dma((2, n_fs, 2)),
            dma((2, n_fs, 2)), dma((2, 2, 2)), dma((2, n_fs)), dma((2, n_fs)), dma((2, 2)),
            dma((4,)), dma((4,)), dma((2, 4)), dma((2, 4)), dma((4,)), dma((4,)),
            dma((owned, 2)), dma((owned, 2)), dma((owned,)), dma((owned,)), dma((owned,)),
        ],
        compiler_params=pltpu.CompilerParams(
            collective_id=0, has_side_effects=True, vmem_limit_bytes=VMEM_BYTES
        ),
        name="fused_layer",
    )(tokens, w_up, w_down, w_in, w_out, pool_w,
      norm_gain.reshape(n_tp, local), ffn_gain.reshape(n_tp, local), packed)
    return result[None]


def fits(n_rep, n_fs, n_tp, args):
    stream, w_in, pool_w, w_down = args[0], args[2], args[4], args[10]
    return (
        n_rep == 2 and n_tp == 2 and n_fs % 4 == 0
        and stream.shape[0] == 1
        and pool_w.shape[0] * GROUP == w_in.shape[1] * n_tp
        and stream.shape[2] * n_tp == w_down.shape[1] * n_fs
    )


def solution(mesh):
    n_rep, n_fs, n_tp = (mesh.shape[name] for name in ("rep", "fs", "tp"))

    def body(*args):
        if fits(n_rep, n_fs, n_tp, args):
            return fused(n_fs, n_tp, *args)
        return on_device(n_rep, n_fs, n_tp, *args)

    return jax.shard_map(
        body,
        mesh=mesh,
        in_specs=(
            P(("rep", "fs"), None, "tp"),
            P(),
            P("fs", "tp"),
            P(("tp", "fs")),
            P(),
            P("fs", "tp"),
            P(("tp", "fs")),
            P(),
            P("fs", "tp"),
            P(("tp", "fs")),
            P("tp", "fs"),
            P("fs"),
        ),
        out_specs=P(("rep", "fs"), None, "tp"),
        check_vma=False,
    )
```

```python
import functools

import jax
import jax.numpy as jnp
from jax import lax
from jax.experimental import pallas as pl
from jax.experimental.pallas import tpu as pltpu
from jax.sharding import PartitionSpec as P

GROUP = 128


epsilon = 0.25
bf16 = jnp.bfloat16
f32 = jnp.float32


def dot(left, right):
    return jnp.dot(left, right, preferred_element_type=f32)


def rms_rows(values, gain):
    floats = values.astype(f32)
    scale = lax.rsqrt(jnp.mean(floats * floats, axis=-1, keepdims=True) + epsilon)
    return (floats * scale * gain).astype(bf16)


def shifted(value, axis_name, count, offset):
    return lax.ppermute(value, axis_name, [(i, (i + offset) % count) for i in range(count)])


def swap_gather(value, axis_name, count, axis):
    index = lax.axis_index(axis_name)
    width = value.shape[axis]
    shape = list(value.shape)
    shape[axis] = width * count
    if count == 2:
        other = shifted(value, axis_name, count, 1)
        low = jnp.where(index == 0, value, other)
        high = jnp.where(index == 0, other, value)
        return jnp.concatenate([low, high], axis=axis)
    full = jnp.zeros(shape, value.dtype)
    full = lax.dynamic_update_slice_in_dim(full, value, index * width, axis)
    for offset in range(1, count):
        piece = shifted(value, axis_name, count, offset)
        origin = (index - offset) % count
        full = lax.dynamic_update_slice_in_dim(full, piece, origin * width, axis)
    return full


def fs_sent(value, factors, offset_a, offset_b):
    n_a, n_b = factors
    pairs = []
    for i in range(n_a * n_b):
        pairs.append((i, ((i // n_b) ^ offset_a) * n_b + ((i % n_b) ^ offset_b)))
    return lax.ppermute(value, "fs", pairs)


def fs_pieces(value, factors):
    n_a, n_b = factors
    rows = [[value] for _ in range(n_a)]
    for x in range(1, n_a):
        rows[x] = [fs_sent(value, factors, x, 0)]
    for y in range(1, n_b):
        for x in range(n_a):
            rows[x].append(fs_sent(rows[x][0], factors, 0, y))
    return rows


def fs_origin(factors, x, y):
    index = lax.axis_index("fs")
    return ((index // factors[1]) ^ x) * factors[1] + ((index % factors[1]) ^ y)


def placed(rows, factors):
    block = rows[0][0].shape[0]
    width = rows[0][0].shape[1]
    full = jnp.zeros((block * factors[0] * factors[1], width), rows[0][0].dtype)
    for y in range(factors[1]):
        for x in range(factors[0]):
            full = lax.dynamic_update_slice_in_dim(
                full, rows[x][y], fs_origin(factors, x, y) * block, 0
            )
    return full


def pool_local(pool_in, first):
    length, width = pool_in.shape
    positions = jnp.arange(length, dtype=jnp.int32)
    source = positions[None, :]
    target = positions[:, None]
    group_of = (first + jnp.arange(width, dtype=jnp.int32)) // GROUP
    means = jnp.zeros((length, width), f32)
    for level in range(4):
        half = 2**level
        band_ones = ((source >= target - half) & (source < target + half)).astype(bf16)
        counts = (jnp.minimum(positions + half, length) - jnp.maximum(positions - half, 0)).astype(f32)
        sums = dot(band_ones, pool_in) / counts[:, None]
        means = jnp.where(group_of[None, :] == level, sums, means)
    return (means - pool_in.astype(f32)).astype(bf16)


def on_device(
    n_rep, n_fs, n_tp,
    stream, norm_gain, w_in, s_in, pool_w, w_out, s_out, ffn_gain, w_up, s_up, w_down, s_down,
):
    rep = lax.axis_index("rep")
    tokens = stream[0]
    length, local_width = tokens.shape
    hidden_width = w_up.shape[1] // n_rep

    n_a = n_tp * max(1, 4 // n_tp)
    factors = (n_a, n_fs // n_a)

    scales = jnp.concatenate([s_in, s_out, s_up, s_down])[None]
    scale_rows = [
        [scales if x == y == 0 else fs_sent(scales, factors, x, y) for y in range(factors[1])]
        for x in range(n_a)
    ]
    scales = placed(scale_rows, factors)
    ends, at = [], 0
    for part in (s_in, s_out, s_up, s_down):
        ends.append(scales[:, at:at + part.shape[0]])
        at += part.shape[0]
    scale_in, scale_out, scale_up = (part.reshape(-1) for part in ends[:3])
    scale_down = ends[3]

    in_rows = fs_pieces(w_in.astype(bf16), factors)
    out_rows = fs_pieces(w_out.astype(bf16), factors)
    w_in_all = placed(in_rows, factors)
    w_out_all = placed(out_rows, factors)

    up_own = lax.dynamic_slice_in_dim(w_up, rep * hidden_width, hidden_width, 1).astype(bf16)
    up_rows = fs_pieces(up_own, factors)
    up_all = placed(up_rows, factors)
    down_own = lax.dynamic_slice_in_dim(w_down, rep * hidden_width, hidden_width, 0).astype(bf16)
    down_own, *_ = lax.optimization_barrier((down_own, *[in_rows[x][0] for x in range(1, n_a)]))
    down_rows = fs_pieces(down_own, factors)

    normed = rms_rows(swap_gather(tokens, "tp", n_tp, 1), norm_gain)
    pool_in = (dot(normed, w_in_all) * scale_in).astype(bf16)
    pooled = pool_local(pool_in, lax.axis_index("tp") * pool_in.shape[1])
    pooled_all = swap_gather(pooled, "tp", n_tp, 1)
    groups = pool_w.shape[0]
    grouped = jnp.einsum(
        "lgc,gcd->lgd", pooled_all.reshape(length, groups, GROUP), pool_w, preferred_element_type=f32
    ).reshape(length, groups * GROUP).astype(bf16)
    mixed = (tokens.astype(f32) + dot(grouped, w_out_all) * scale_out).astype(bf16)

    mixed_own = swap_gather(mixed, "tp", n_tp, 1)
    sequences = [mixed_own]
    for offset in range(1, n_rep):
        other = shifted(mixed, "rep", n_rep, offset)
        sequences.append(swap_gather(other, "tp", n_tp, 1))
    scale_hidden = lax.dynamic_slice_in_dim(scale_up, rep * hidden_width, hidden_width, 0)
    hidden = []
    for rows in sequences:
        rows = rms_rows(rows, ffn_gain)
        upward = dot(rows, up_all)
        hidden.append(jnp.square(jax.nn.relu(upward * scale_hidden)).astype(bf16))

    hidden = jnp.concatenate(hidden, axis=0)
    width = w_down.shape[1]
    per_tp = n_a // n_tp
    tp = lax.axis_index("tp")
    turn = ((lax.axis_index("fs") // factors[1]) // per_tp) ^ tp
    result = jnp.zeros((length, local_width), bf16)
    for y in range(factors[1]):
        for xi in range(per_tp):
            stacked = jnp.stack([down_rows[xt * per_tp + xi][y] for xt in range(n_tp)])
            blocks, block_scales = [], []
            for k in range(n_tp):
                blocks.append(lax.dynamic_index_in_dim(stacked, turn ^ k, 0, keepdims=False))
                origin = fs_origin(factors, xi, y) ^ ((turn ^ k) * per_tp * factors[1])
                block_scales.append(lax.dynamic_index_in_dim(scale_down, origin, 0, keepdims=False))
            both = jnp.concatenate(blocks, axis=1)
            partial = (dot(hidden, both) * jnp.concatenate(block_scales)).astype(bf16)
            total = partial[:, :width].astype(f32)
            for k in range(1, n_tp):
                pairs = [(i, i ^ k) for i in range(n_tp)]
                total = total + lax.ppermute(partial[:, k * width:(k + 1) * width], "tp", pairs).astype(f32)
            own = total[:length]
            for k in range(1, n_rep):
                back = shifted(total[k * length:(k + 1) * length].astype(bf16), "rep", n_rep, -k)
                own = own + back.astype(f32)
            inner = (fs_origin(factors, xi, y) % (per_tp * factors[1])) * width
            mixed_part = lax.dynamic_slice_in_dim(mixed, inner, width, 1)
            piece = (mixed_part.astype(f32) + own).astype(bf16)
            result = lax.dynamic_update_slice_in_dim(result, piece, inner, 1)
    return result[None]


UP_TILE = (512, 512)
DOWN_ROWS = 512
PARTS = 2
MESH = pl.DeviceIdType.MESH
VMEM_BYTES = 67_043_328


def fused_kernel(
    n_fs, n_tp,
    stream, w_up, w_down, w_in, w_out, pool_w, norm_gain, ffn_gain, own_scales,
    out,
    up_all, down_all, up_other, down_other, ffn_rows, hidden, mixed, in_all, out_all,
    pool_in, grouped, squares, core_got, core_sent, pair_got, pair_sent, totals, pair_total,
    up_floats, scales, scale_in, scale_out, scale_up,
    load_sem, scale_send, scale_recv,
    mix_recv, mix_own_send, mix_z_send, mix_x_send, mix_y_send,
    piece_recv, own_send, z_send, x_send, y_send,
    core_send, core_recv, act_core_send, act_core_recv, act_pair_send, act_pair_recv,
    part_core_send, part_core_recv, part_pair_send, part_pair_recv, store_sem,
):
    rep, fs, tp = lax.axis_index("rep"), lax.axis_index("fs"), lax.axis_index("tp")
    n_z = n_fs // 2
    z, y = fs // 2, fs % 2
    length, local = stream.shape
    width = n_tp * local
    units = up_all.shape[1]
    block = down_all.shape[2]
    owned = n_fs // n_tp
    in_rows, out_rows = w_in.shape[0], w_out.shape[0]
    pool_width = pool_in.shape[1]
    core, across, pair = {"tp": 1 - tp}, {"rep": 1 - rep}, {"fs": fs + 1 - 2 * y}

    def remote(ref, there, sent, got, device):
        return pltpu.make_async_remote_copy(
            src_ref=ref, dst_ref=there, send_sem=sent, recv_sem=got,
            device_id=device, device_id_type=MESH,
        )

    def at_step(i):
        j, other = i // 2, i % 2
        both = jnp.minimum(z, n_z - 1 - z)
        paired = j <= 2 * both
        distance = jnp.where(paired, (j + 1) // 2, j - both)
        left = jnp.where(paired, j % 2 == 1, z > n_z - 1 - z)
        source = z + jnp.where(left, -distance, distance)
        return source * 2 + y + other - 2 * y * other, left

    def onward(left):
        return jnp.where(left, z < n_z - 1, z > 0), {"fs": fs + jnp.where(left, 2, -2)}

    up_piece, down_piece = up_other.shape[0] // (2 * PARTS), units // (2 * PARTS)

    def piece(kind, source, half, q):
        place = half * PARTS + q
        if kind == 0:
            start = (source * 2 * PARTS + place) * up_piece
            return up_all.at[pl.ds(pl.multiple_of(start, up_piece), up_piece), :]
        return down_all.at[source, pl.ds(pl.multiple_of(place * down_piece, down_piece), down_piece), :]

    def mix_piece(kind, source, half):
        ref, rows = ((in_all, in_rows), (out_all, out_rows))[kind]
        return ref.at[pl.ds(pl.multiple_of(source * rows + half * (rows // 2), rows // 2), rows // 2), :]

    def own_copy(kind, order, side, q):
        source = fs if order == 0 else fs + 1 - 2 * y
        ref = piece(kind, source, rep, q)
        return remote(ref, ref, own_send.at[kind, side, order, q], piece_recv.at[kind, source, rep, q],
                      {"fs": fs + (2 if side == 0 else -2)})

    def pair_copy(kind, half, q):
        size = (up_piece, down_piece)[kind]
        ref = (up_other, down_other)[kind].at[pl.ds(pl.multiple_of((half * PARTS + q) * size, size), size), :]
        return remote(ref, piece(kind, fs, half, q), y_send.at[kind, half, q], piece_recv.at[kind, fs, half, q], pair)

    def onward_copy(kind, source, q, device):
        ref = piece(kind, source, rep, q)
        return remote(ref, ref, z_send.at[kind, source, q], piece_recv.at[kind, source, rep, q], device)

    def across_copy(kind, source, q):
        ref = piece(kind, source, rep, q)
        return remote(ref, ref, x_send.at[kind, source, q], piece_recv.at[kind, source, rep, q], across)

    def piece_wait(kind, source, half, q):
        ref = piece(kind, source, half, q)
        remote(ref, ref, x_send.at[kind, source, q], piece_recv.at[kind, source, half, q], across).wait_recv()

    def other_half(kind, source):
        for q in range(PARTS):
            piece_wait(kind, source, 1 - rep, q)

    def both_sides(act):
        @pl.when(z < n_z - 1)
        def _():
            act(0)

        @pl.when(z > 0)
        def _():
            act(1)

    def send_own(kind, q):
        both_sides(lambda side: own_copy(kind, 0, side, q).start())

    def send_pair(kind):
        for turn in range(2):
            for q in range(PARTS):
                pair_copy(kind, rep + turn - 2 * rep * turn, q).start()

    def pass_pair(kind):
        for q in range(PARTS):
            piece_wait(kind, fs + 1 - 2 * y, rep, q)
            both_sides(lambda side, q=q: own_copy(kind, 1, side, q).start())

    def pass_on(kind, i):
        source, left = at_step(i)
        going, device = onward(left)
        for q in range(PARTS):
            piece_wait(kind, source, rep, q)

            @pl.when(going)
            def _():
                onward_copy(kind, source, q, device).start()

            across_copy(kind, source, q).start()

    def mix_own_copy(kind, side):
        ref = mix_piece(kind, fs, rep)
        return remote(ref, ref, mix_own_send.at[kind, side], mix_recv.at[kind, fs, rep],
                      {"fs": fs + (2 if side == 0 else -2)})

    def mix_onward_copy(kind, source, device):
        ref = mix_piece(kind, source, rep)
        return remote(ref, ref, mix_z_send.at[kind, source], mix_recv.at[kind, source, rep], device)

    def mix_across_copy(kind, source):
        ref = mix_piece(kind, source, rep)
        return remote(ref, ref, mix_x_send.at[kind, source], mix_recv.at[kind, source, rep], across)

    def mix_pair_copy(kind, source, half):
        ref = mix_piece(kind, source, half)
        return remote(ref, ref, mix_y_send.at[kind, source, half], mix_recv.at[kind, source, half], pair)

    def mix_wait(kind, source, half):
        mix_pair_copy(kind, source, half).wait_recv()

    def scale_copy(offset):
        return remote(own_scales, scales.at[fs], scale_send.at[offset], scale_recv.at[fs],
                      {"fs": lax.rem(fs + offset, n_fs)})

    def core_copy(which, ref, there):
        return remote(ref, there, core_send.at[which], core_recv.at[which], core)

    my_half = pl.ds(pl.multiple_of(tp * local, local), local)
    my_pool = pl.ds(pl.multiple_of(tp * pool_width, pool_width), pool_width)
    n_tiles = 4
    tile = length // n_tiles

    def rows_of(t):
        return pl.ds(pl.multiple_of(t * tile, tile), tile)

    def act_pair_copy(t):
        return remote(ffn_rows.at[0, rows_of(t), my_half], ffn_rows.at[1, rows_of(t), my_half],
                      act_pair_send.at[t], act_pair_recv.at[t], pair)

    def act_core_copy(which, t):
        ref = ffn_rows.at[which, rows_of(t), my_half]
        return remote(ref, ref, act_core_send.at[which, t], act_core_recv.at[which, t], core)

    load_tokens = pltpu.make_async_copy(stream, mixed, load_sem.at[0])

    def load_up(which, half):
        return pltpu.make_async_copy(
            w_up.at[:, pl.ds(pl.multiple_of(half * units, units), units)], up_floats, load_sem.at[1 + which])

    quarter = units // 2

    def load_down(q):
        return pltpu.make_async_copy(
            w_down.at[pl.ds(q * quarter, quarter), :], totals.at[q], load_sem.at[3 + q])

    load_tokens.start()
    load_up(0, y).start()
    for q in range(4):
        load_down(q).start()

    own_in = pl.ds(pl.multiple_of(fs * in_rows, in_rows), in_rows)
    own_out = pl.ds(pl.multiple_of(fs * out_rows, out_rows), out_rows)
    in_all[own_in, :] = w_in[...].astype(bf16)
    out_all[own_out, :] = w_out[...].astype(bf16)

    barrier = pltpu.get_barrier_semaphore()
    for offset in range(1, n_fs):
        pl.semaphore_signal(barrier, inc=1, device_id={"fs": lax.rem(fs + offset, n_fs)}, device_id_type=MESH)
    pl.semaphore_signal(barrier, inc=1, device_id=across, device_id_type=MESH)
    pl.semaphore_signal(barrier, inc=1, device_id=core, device_id_type=MESH)

    pieces = 8
    up_tile = up_floats.shape[0] // pieces

    def cast_own(t, carry):
        rows = pl.ds(pl.multiple_of(t * up_tile, up_tile), up_tile)
        there = pl.ds(pl.multiple_of(fs * up_floats.shape[0] + t * up_tile, up_tile), up_tile)
        up_all[there, :] = up_floats[rows, :].astype(bf16)
        return carry

    def cast_other(t, carry):
        rows = pl.ds(pl.multiple_of(t * up_tile, up_tile), up_tile)
        up_other[rows, :] = up_floats[rows, :].astype(bf16)
        return carry

    def square_rows(t, carry):
        floats = mixed[rows_of(t), :].astype(f32)
        total = jnp.sum(floats * floats, axis=1, keepdims=True)
        squares[0, rows_of(t), :] = jnp.broadcast_to(total, (tile, 128))
        return carry

    load_up(0, y).wait()
    lax.fori_loop(0, pieces, cast_own, 0)
    load_up(1, 1 - y).start()
    load_tokens.wait()
    lax.fori_loop(0, n_tiles, square_rows, 0)
    pl.semaphore_wait(barrier, n_fs + 1)

    for kind in range(2):
        both_sides(lambda side, kind=kind: mix_own_copy(kind, side).start())
        for half in range(2):
            mix_pair_copy(kind, fs, half).start()
    for offset in range(1, n_fs):
        scale_copy(offset).start()
    share_squares = core_copy(0, squares.at[0], squares.at[1])
    share_squares.start()
    scales[fs] = own_scales[...]

    def mix_step(j):
        source, left = at_step(2 * j)
        going, device = onward(left)
        for kind in range(2):
            mix_wait(kind, source, rep)

            @pl.when(going)
            def _():
                mix_onward_copy(kind, source, device).start()

            mix_across_copy(kind, source).start()
            mix_pair_copy(kind, source, rep).start()

    load_up(1, 1 - y).wait()
    lax.fori_loop(0, pieces, cast_other, 0)
    share_squares.wait()

    def normed_rows(t, carry):
        rows = rows_of(t)
        total = squares[0, rows, :] + squares[1, rows, :]
        scale = lax.rsqrt(total[:, :1] * (1.0 / width) + epsilon)
        floats = mixed[rows, :].astype(f32)
        hidden[1, rows, my_half] = (floats * scale * norm_gain[pl.ds(tp, 1), :]).astype(bf16)
        return carry

    lax.fori_loop(0, n_tiles, normed_rows, 0)
    share_normed = core_copy(1, hidden.at[1, :, my_half], hidden.at[1, :, my_half])
    share_normed.start()

    for j in range(1, n_z):
        mix_step(j)
    for q in range(PARTS):
        send_own(0, q)

    for q in range(4):
        load_down(q).wait()
    down_tile = quarter // pieces

    def cast_down(t, carry):
        rows = pl.ds(pl.multiple_of(t * down_tile, down_tile), down_tile)
        for half in range(2):
            there = pl.ds(pl.multiple_of(half * quarter + t * down_tile, down_tile), down_tile)
            down_all[fs, there, :] = totals[2 * y + half, rows, :].astype(bf16)
            down_other[there, :] = totals[2 - 2 * y + half, rows, :].astype(bf16)
        return carry

    inner = jnp.minimum(z, n_z - 1 - z) > 0

    def inner_pass(kind, i):
        @pl.when(inner)
        def _():
            pass_on(kind, i)

    def outer_pass(kind, i):
        @pl.when(jnp.logical_not(inner))
        def _():
            pass_on(kind, i)

    for j in range(1, n_z):
        source, _ = at_step(2 * j)
        for kind in range(2):
            mix_wait(kind, source, 1 - rep)
            mix_pair_copy(kind, source, 1 - rep).start()
    send_pair(0)
    lax.fori_loop(0, pieces, cast_down, 0)
    for q in range(PARTS):
        send_own(1, q)
    pass_on(0, 2)
    inner_pass(0, 4)

    for offset in range(1, n_fs):
        source = lax.rem(fs + offset, n_fs)
        remote(own_scales, scales.at[source], scale_send.at[offset], scale_recv.at[source], pair).wait_recv()
    gathered = scales[...]
    summed = jnp.sum(gathered[:, 0:2, :], axis=0)
    scale_in[...] = jnp.concatenate([summed[0:1], summed[1:2]], axis=1)
    for source in range(n_fs):
        scale_out[:, source * 128:(source + 1) * 128] = gathered[source, 2:3, :]
    per = units // (n_fs // 2)
    for q in range(n_fs // 2):
        rows = scales[y * (n_fs // 2) + q]
        for i in range(per // 128):
            scale_up[:, q * per + i * 128:q * per + (i + 1) * 128] = rows[3 + i:4 + i, :]

    for source_z in range(n_z):
        for kind in range(2):
            for half in range(2):
                mix_wait(kind, source_z * 2 + 1 - y, half)

    share_normed.wait()

    def pool_rows(t, carry):
        rows = rows_of(t)
        product = jnp.dot(hidden[1, rows, :], in_all[...], preferred_element_type=f32)
        pool_in[rows, :] = (product * scale_in[...]).astype(bf16)
        return carry

    lax.fori_loop(0, n_tiles, pool_rows, 0)
    per_core = pool_width // GROUP

    def group_rows(t, carry):
        rows = rows_of(t)
        target = lax.broadcasted_iota(jnp.int32, (tile, length), 0) + t * tile
        source = lax.broadcasted_iota(jnp.int32, (tile, length), 1)
        gap = source - target
        at = lax.broadcasted_iota(jnp.int32, (tile, GROUP), 0) + t * tile
        for g in range(per_core):
            half = jnp.left_shift(jnp.int32(1), tp * per_core + g)
            lanes = slice(g * GROUP, (g + 1) * GROUP)
            band = jnp.where((gap >= -half) & (gap < half), 1.0, 0.0).astype(bf16)
            sums = jnp.dot(band, pool_in[:, lanes], preferred_element_type=f32)
            counts = (jnp.minimum(at + half, length) - jnp.maximum(at - half, 0)).astype(f32)
            pooled = (sums / counts - pool_in[rows, lanes].astype(f32)).astype(bf16)
            product = jnp.dot(pooled, pool_w[tp * per_core + g], preferred_element_type=f32)
            there = pl.ds(pl.multiple_of(tp * pool_width + g * GROUP, GROUP), GROUP)
            grouped[rows, there] = product.astype(bf16)
        return carry

    lax.fori_loop(0, n_tiles, group_rows, 0)
    share_grouped = core_copy(2, grouped.at[:, my_pool], grouped.at[:, my_pool])
    share_grouped.start()
    outer_pass(1, 2)
    pass_pair(0)
    share_grouped.wait()

    def mix_rows(t, carry):
        rows = rows_of(t)
        product = jnp.dot(grouped[rows, :], out_all[...], preferred_element_type=f32)
        total = (mixed[rows, :].astype(f32) + product * scale_out[...]).astype(bf16)
        mixed[rows, :] = total
        floats = total.astype(f32)
        squares[0, rows, :] = jnp.broadcast_to(jnp.sum(floats * floats, axis=1, keepdims=True), (tile, 128))
        return carry

    lax.fori_loop(0, n_tiles, mix_rows, 0)
    share_more = core_copy(3, squares.at[0], squares.at[1])
    share_more.start()
    inner_pass(0, 6)
    outer_pass(0, 4)
    share_more.wait()

    def ffn_in_rows(t, carry):
        rows = rows_of(t)
        total = squares[0, rows, :] + squares[1, rows, :]
        scale = lax.rsqrt(total[:, :1] * (1.0 / width) + epsilon)
        floats = mixed[rows, :].astype(f32)
        ffn_rows[0, rows, my_half] = (floats * scale * ffn_gain[pl.ds(tp, 1), :]).astype(bf16)
        act_pair_copy(t).start()
        act_core_copy(0, t).start()
        return carry

    lax.fori_loop(0, n_tiles, ffn_in_rows, 0)
    send_pair(1)

    pass_on(0, 3)
    outer_pass(0, 6)
    pass_on(0, 5)
    pass_on(0, 7)
    inner_pass(1, 2)
    inner_pass(1, 4)
    inner_pass(1, 6)
    other_half(0, fs + 1 - 2 * y)

    def up_ready(i, carry):
        source, _ = at_step(i)
        other_half(0, source)
        return carry

    lax.fori_loop(2, 2 * n_z, up_ready, 0)
    for t in range(n_tiles):
        act_core_copy(0, t).wait_recv()

    up_rows, up_columns = UP_TILE
    n_rows, n_columns = length // up_rows, units // up_columns
    half_tiles = n_rows * n_columns // 2

    def up_tiles(sequence):
        def body(n, carry):
            rows = pl.ds(pl.multiple_of((n % n_rows) * up_rows, up_rows), up_rows)
            columns = pl.ds(pl.multiple_of((n // n_rows) * up_columns, up_columns), up_columns)
            product = jnp.dot(ffn_rows[sequence, rows, :], up_all[:, columns], preferred_element_type=f32)
            positive = jnp.maximum(product * scale_up[:, columns], 0.0)
            hidden[sequence, rows, columns] = (positive * positive).astype(bf16)
            return carry

        return body

    for t in range(n_tiles):
        act_pair_copy(t).wait_recv()
        act_core_copy(1, t).start()
    lax.fori_loop(0, half_tiles, up_tiles(0), 0)
    outer_pass(1, 4)
    lax.fori_loop(half_tiles, 2 * half_tiles, up_tiles(0), 0)
    pass_pair(1)
    for t in range(n_tiles):
        act_core_copy(1, t).wait_recv()
    lax.fori_loop(0, half_tiles, up_tiles(1), 0)
    outer_pass(1, 6)
    lax.fori_loop(half_tiles, 2 * half_tiles, up_tiles(1), 0)

    down_rows = DOWN_ROWS

    def part_core_copy(index, sequence):
        span = pl.ds(sequence * length, length)
        return remote(core_sent.at[index, span, :], core_got.at[index, span, :],
                      part_core_send.at[index, sequence], part_core_recv.at[index, sequence], core)

    def part_pair_copy(index):
        return remote(pair_sent.at[index], pair_got.at[index],
                      part_pair_send.at[index], part_pair_recv.at[index], pair)

    def down_order(n):
        return jnp.where(n < n_z, 2 * n, 2 * (n - n_z) + 1)

    def down_block(n, carry):
        @pl.when(inner & (n >= 1) & (n < n_z - 1))
        def _():
            pass_on(1, 2 * n + 1)

        @pl.when(jnp.logical_not(inner) & (n % 2 == 1) & (n < 2 * n_z - 4))
        def _():
            pass_on(1, n + 2)

        @pl.when(n == 2 * n_z - 3)
        def _():
            pass_on(1, 2 * n_z - 1)

        source, _ = at_step(down_order(n))

        @pl.when(n > 0)
        def _():
            other_half(1, source)

        index = source % owned
        mine = source // owned == tp
        scale = jnp.concatenate([scales[source, 7:8, :], scales[source, 8:9, :]], axis=1)
        for sequence in (1, 0):
            def down_tile_rows(m, inner):
                rows = pl.ds(pl.multiple_of(m * down_rows, down_rows), down_rows)
                product = jnp.dot(hidden[sequence, rows, :], down_all[source], preferred_element_type=f32) * scale

                @pl.when(mine)
                def _():
                    if sequence == 1:
                        pair_total[rows, :] = product
                    else:
                        totals[index, rows, :] = product

                @pl.when(jnp.logical_not(mine))
                def _():
                    there = pl.ds(pl.multiple_of(sequence * length + m * down_rows, down_rows), down_rows)
                    core_sent[index, there, :] = product.astype(bf16)

                return inner

            lax.fori_loop(0, length // down_rows, down_tile_rows, 0)

            @pl.when(jnp.logical_not(mine))
            def _():
                part_core_copy(index, sequence).start()

        @pl.when(mine)
        def _():
            part_core_copy(index, 1).wait_recv()
            pair_sent[index] = (pair_total[...] + core_got[index, length:2 * length, :].astype(f32)).astype(bf16)
            part_pair_copy(index).start()

        return carry

    lax.fori_loop(0, n_fs, down_block, 0)

    def store_block(index):
        columns = pl.ds(pl.multiple_of(index * block, block), block)
        return pltpu.make_async_copy(pair_sent.at[index], out.at[:, columns], store_sem.at[index])

    def finish_block(i, carry):
        source, _ = at_step(down_order(i))

        @pl.when(source // owned == tp)
        def _():
            index = source % owned
            columns = pl.ds(pl.multiple_of(index * block, block), block)
            part_core_copy(index, 0).wait_recv()
            part_pair_copy(index).wait()
            total = totals[index] + core_got[index, 0:length, :].astype(f32) + pair_got[index].astype(f32)
            pair_sent[index] = (mixed[:, columns].astype(f32) + total).astype(bf16)
            store_block(index).start()

        return carry

    lax.fori_loop(0, n_fs, finish_block, 0)

    for kind in range(2):
        both_sides(lambda side, kind=kind: mix_own_copy(kind, side).wait_send())
        for q in range(PARTS):
            for order in range(2):
                both_sides(lambda side, kind=kind, order=order, q=q: own_copy(kind, order, side, q).wait_send())
            for half in range(2):
                pair_copy(kind, half, q).wait_send()
        for half in range(2):
            mix_pair_copy(kind, fs, half).wait_send()

        def sent_step(i, carry, kind=kind):
            source, left = at_step(i)
            going, device = onward(left)

            for q in range(PARTS):
                @pl.when(going)
                def _():
                    onward_copy(kind, source, q, device).wait_send()

                across_copy(kind, source, q).wait_send()

            @pl.when(i % 2 == 0)
            def _():
                @pl.when(going)
                def _():
                    mix_onward_copy(kind, source, device).wait_send()

                mix_across_copy(kind, source).wait_send()
                mix_pair_copy(kind, source, 0).wait_send()
                mix_pair_copy(kind, source, 1).wait_send()

            return carry

        lax.fori_loop(2, 2 * n_z, sent_step, 0)
    for offset in range(1, n_fs):
        scale_copy(offset).wait_send()
    for t in range(n_tiles):
        act_pair_copy(t).wait_send()
        for which in range(2):
            act_core_copy(which, t).wait_send()
    for index in range(owned):
        for sequence in range(2):
            part_core_copy(index, sequence).wait_send()
        store_block(index).wait()


def fused(n_fs, n_tp, stream, norm_gain, w_in, s_in, pool_w, w_out, s_out,
          ffn_gain, w_up, s_up, w_down, s_down):
    fs = lax.axis_index("fs")
    tokens = stream[0]
    length, local = tokens.shape
    rows, all_units = w_up.shape
    units = all_units // 2
    block = w_down.shape[1]
    in_rows, pool_width = w_in.shape
    out_rows = w_out.shape[0]
    owned = n_fs // n_tp
    placed_in = lax.dynamic_update_slice(jnp.zeros((pool_width,), f32), s_in, (fs * s_in.shape[0],))
    packed = jnp.concatenate([placed_in, s_out, s_up, s_down])
    packed = jnp.pad(packed, (0, 16 * 128 - packed.shape[0])).reshape(16, 128)
    vmem, anywhere = pl.BlockSpec(memory_space=pltpu.VMEM), pl.BlockSpec(memory_space=pl.ANY)
    dma = pltpu.SemaphoreType.DMA
    result = pl.pallas_call(
        functools.partial(fused_kernel, n_fs, n_tp),
        out_shape=jax.ShapeDtypeStruct((length, local), bf16),
        in_specs=[anywhere] * 3 + [vmem] * 6,
        out_specs=anywhere,
        scratch_shapes=[
            pltpu.VMEM((rows * n_fs, units), bf16),
            pltpu.VMEM((n_fs, units, block), bf16),
            pltpu.VMEM((rows, units), bf16),
            pltpu.VMEM((units, block), bf16),
            pltpu.VMEM((2, length, n_tp * local), bf16),
            pltpu.VMEM((2, length, units), bf16),
            pltpu.VMEM((length, local), bf16),
            pltpu.VMEM((in_rows * n_fs, pool_width), bf16),
            pltpu.VMEM((out_rows * n_fs, local), bf16),
            pltpu.VMEM((length, pool_width), bf16),
            pltpu.VMEM((length, n_tp * pool_width), bf16),
            pltpu.VMEM((2, length, 128), f32),
            pltpu.VMEM((owned, 2 * length, block), bf16),
            pltpu.VMEM((owned, 2 * length, block), bf16),
            pltpu.VMEM((owned, length, block), bf16),
            pltpu.VMEM((owned, length, block), bf16),
            pltpu.VMEM((owned, length, block), f32),
            pltpu.VMEM((length, block), f32),
            pltpu.VMEM((rows, units), f32),
            pltpu.VMEM((n_fs, 16, 128), f32),
            pltpu.VMEM((1, pool_width), f32),
            pltpu.VMEM((1, local), f32),
            pltpu.VMEM((1, units), f32),
            dma((7,)), dma((n_fs,)), dma((n_fs,)),
            dma((2, n_fs, 2)), dma((2, 2)), dma((2, n_fs)), dma((2, n_fs)), dma((2, n_fs, 2)),
            dma((2, n_fs, 2, PARTS)), dma((2, 2, 2, PARTS)), dma((2, n_fs, PARTS)), dma((2, n_fs, PARTS)),
            dma((2, 2, PARTS)),
            dma((4,)), dma((4,)), dma((2, 4)), dma((2, 4)), dma((4,)), dma((4,)),
            dma((owned, 2)), dma((owned, 2)), dma((owned,)), dma((owned,)), dma((owned,)),
        ],
        compiler_params=pltpu.CompilerParams(
            collective_id=0, has_side_effects=True, vmem_limit_bytes=VMEM_BYTES
        ),
        name="fused_layer",
    )(tokens, w_up, w_down, w_in, w_out, pool_w,
      norm_gain.reshape(n_tp, local), ffn_gain.reshape(n_tp, local), packed)
    return result[None]


def fits(n_rep, n_fs, n_tp, args):
    stream, w_in, pool_w, w_down = args[0], args[2], args[4], args[10]
    return (
        n_rep == 2 and n_tp == 2 and n_fs % 4 == 0
        and stream.shape[0] == 1
        and pool_w.shape[0] * GROUP == w_in.shape[1] * n_tp
        and stream.shape[2] * n_tp == w_down.shape[1] * n_fs
    )


def solution(mesh):
    n_rep, n_fs, n_tp = (mesh.shape[name] for name in ("rep", "fs", "tp"))

    def body(*args):
        if fits(n_rep, n_fs, n_tp, args):
            return fused(n_fs, n_tp, *args)
        return on_device(n_rep, n_fs, n_tp, *args)

    return jax.shard_map(
        body,
        mesh=mesh,
        in_specs=(
            P(("rep", "fs"), None, "tp"),
            P(),
            P("fs", "tp"),
            P(("tp", "fs")),
            P(),
            P("fs", "tp"),
            P(("tp", "fs")),
            P(),
            P("fs", "tp"),
            P(("tp", "fs")),
            P("tp", "fs"),
            P("fs"),
        ),
        out_specs=P(("rep", "fs"), None, "tp"),
        check_vma=False,
    )
```

```python
import functools

import jax
import jax.numpy as jnp
from jax import lax
from jax.experimental import pallas as pl
from jax.experimental.pallas import tpu as pltpu
from jax.sharding import PartitionSpec as P

GROUP = 128


epsilon = 0.25
bf16 = jnp.bfloat16
f32 = jnp.float32


def dot(left, right):
    return jnp.dot(left, right, preferred_element_type=f32)


def rms_rows(values, gain):
    floats = values.astype(f32)
    scale = lax.rsqrt(jnp.mean(floats * floats, axis=-1, keepdims=True) + epsilon)
    return (floats * scale * gain).astype(bf16)


def shifted(value, axis_name, count, offset):
    return lax.ppermute(value, axis_name, [(i, (i + offset) % count) for i in range(count)])


def swap_gather(value, axis_name, count, axis):
    index = lax.axis_index(axis_name)
    width = value.shape[axis]
    shape = list(value.shape)
    shape[axis] = width * count
    if count == 2:
        other = shifted(value, axis_name, count, 1)
        low = jnp.where(index == 0, value, other)
        high = jnp.where(index == 0, other, value)
        return jnp.concatenate([low, high], axis=axis)
    full = jnp.zeros(shape, value.dtype)
    full = lax.dynamic_update_slice_in_dim(full, value, index * width, axis)
    for offset in range(1, count):
        piece = shifted(value, axis_name, count, offset)
        origin = (index - offset) % count
        full = lax.dynamic_update_slice_in_dim(full, piece, origin * width, axis)
    return full


def fs_sent(value, factors, offset_a, offset_b):
    n_a, n_b = factors
    pairs = []
    for i in range(n_a * n_b):
        pairs.append((i, ((i // n_b) ^ offset_a) * n_b + ((i % n_b) ^ offset_b)))
    return lax.ppermute(value, "fs", pairs)


def fs_pieces(value, factors):
    n_a, n_b = factors
    rows = [[value] for _ in range(n_a)]
    for x in range(1, n_a):
        rows[x] = [fs_sent(value, factors, x, 0)]
    for y in range(1, n_b):
        for x in range(n_a):
            rows[x].append(fs_sent(rows[x][0], factors, 0, y))
    return rows


def fs_origin(factors, x, y):
    index = lax.axis_index("fs")
    return ((index // factors[1]) ^ x) * factors[1] + ((index % factors[1]) ^ y)


def placed(rows, factors):
    block = rows[0][0].shape[0]
    width = rows[0][0].shape[1]
    full = jnp.zeros((block * factors[0] * factors[1], width), rows[0][0].dtype)
    for y in range(factors[1]):
        for x in range(factors[0]):
            full = lax.dynamic_update_slice_in_dim(
                full, rows[x][y], fs_origin(factors, x, y) * block, 0
            )
    return full


def pool_local(pool_in, first):
    length, width = pool_in.shape
    positions = jnp.arange(length, dtype=jnp.int32)
    source = positions[None, :]
    target = positions[:, None]
    group_of = (first + jnp.arange(width, dtype=jnp.int32)) // GROUP
    means = jnp.zeros((length, width), f32)
    for level in range(4):
        half = 2**level
        band_ones = ((source >= target - half) & (source < target + half)).astype(bf16)
        counts = (jnp.minimum(positions + half, length) - jnp.maximum(positions - half, 0)).astype(f32)
        sums = dot(band_ones, pool_in) / counts[:, None]
        means = jnp.where(group_of[None, :] == level, sums, means)
    return (means - pool_in.astype(f32)).astype(bf16)


def on_device(
    n_rep, n_fs, n_tp,
    stream, norm_gain, w_in, s_in, pool_w, w_out, s_out, ffn_gain, w_up, s_up, w_down, s_down,
):
    rep = lax.axis_index("rep")
    tokens = stream[0]
    length, local_width = tokens.shape
    hidden_width = w_up.shape[1] // n_rep

    n_a = n_tp * max(1, 4 // n_tp)
    factors = (n_a, n_fs // n_a)

    scales = jnp.concatenate([s_in, s_out, s_up, s_down])[None]
    scale_rows = [
        [scales if x == y == 0 else fs_sent(scales, factors, x, y) for y in range(factors[1])]
        for x in range(n_a)
    ]
    scales = placed(scale_rows, factors)
    ends, at = [], 0
    for part in (s_in, s_out, s_up, s_down):
        ends.append(scales[:, at:at + part.shape[0]])
        at += part.shape[0]
    scale_in, scale_out, scale_up = (part.reshape(-1) for part in ends[:3])
    scale_down = ends[3]

    in_rows = fs_pieces(w_in.astype(bf16), factors)
    out_rows = fs_pieces(w_out.astype(bf16), factors)
    w_in_all = placed(in_rows, factors)
    w_out_all = placed(out_rows, factors)

    up_own = lax.dynamic_slice_in_dim(w_up, rep * hidden_width, hidden_width, 1).astype(bf16)
    up_rows = fs_pieces(up_own, factors)
    up_all = placed(up_rows, factors)
    down_own = lax.dynamic_slice_in_dim(w_down, rep * hidden_width, hidden_width, 0).astype(bf16)
    down_own, *_ = lax.optimization_barrier((down_own, *[in_rows[x][0] for x in range(1, n_a)]))
    down_rows = fs_pieces(down_own, factors)

    normed = rms_rows(swap_gather(tokens, "tp", n_tp, 1), norm_gain)
    pool_in = (dot(normed, w_in_all) * scale_in).astype(bf16)
    pooled = pool_local(pool_in, lax.axis_index("tp") * pool_in.shape[1])
    pooled_all = swap_gather(pooled, "tp", n_tp, 1)
    groups = pool_w.shape[0]
    grouped = jnp.einsum(
        "lgc,gcd->lgd", pooled_all.reshape(length, groups, GROUP), pool_w, preferred_element_type=f32
    ).reshape(length, groups * GROUP).astype(bf16)
    mixed = (tokens.astype(f32) + dot(grouped, w_out_all) * scale_out).astype(bf16)

    mixed_own = swap_gather(mixed, "tp", n_tp, 1)
    sequences = [mixed_own]
    for offset in range(1, n_rep):
        other = shifted(mixed, "rep", n_rep, offset)
        sequences.append(swap_gather(other, "tp", n_tp, 1))
    scale_hidden = lax.dynamic_slice_in_dim(scale_up, rep * hidden_width, hidden_width, 0)
    hidden = []
    for rows in sequences:
        rows = rms_rows(rows, ffn_gain)
        upward = dot(rows, up_all)
        hidden.append(jnp.square(jax.nn.relu(upward * scale_hidden)).astype(bf16))

    hidden = jnp.concatenate(hidden, axis=0)
    width = w_down.shape[1]
    per_tp = n_a // n_tp
    tp = lax.axis_index("tp")
    turn = ((lax.axis_index("fs") // factors[1]) // per_tp) ^ tp
    result = jnp.zeros((length, local_width), bf16)
    for y in range(factors[1]):
        for xi in range(per_tp):
            stacked = jnp.stack([down_rows[xt * per_tp + xi][y] for xt in range(n_tp)])
            blocks, block_scales = [], []
            for k in range(n_tp):
                blocks.append(lax.dynamic_index_in_dim(stacked, turn ^ k, 0, keepdims=False))
                origin = fs_origin(factors, xi, y) ^ ((turn ^ k) * per_tp * factors[1])
                block_scales.append(lax.dynamic_index_in_dim(scale_down, origin, 0, keepdims=False))
            both = jnp.concatenate(blocks, axis=1)
            partial = (dot(hidden, both) * jnp.concatenate(block_scales)).astype(bf16)
            total = partial[:, :width].astype(f32)
            for k in range(1, n_tp):
                pairs = [(i, i ^ k) for i in range(n_tp)]
                total = total + lax.ppermute(partial[:, k * width:(k + 1) * width], "tp", pairs).astype(f32)
            own = total[:length]
            for k in range(1, n_rep):
                back = shifted(total[k * length:(k + 1) * length].astype(bf16), "rep", n_rep, -k)
                own = own + back.astype(f32)
            inner = (fs_origin(factors, xi, y) % (per_tp * factors[1])) * width
            mixed_part = lax.dynamic_slice_in_dim(mixed, inner, width, 1)
            piece = (mixed_part.astype(f32) + own).astype(bf16)
            result = lax.dynamic_update_slice_in_dim(result, piece, inner, 1)
    return result[None]


LANES = 128
UP_TILE = (512, 512)
DOWN_ROWS = 512
PARTS = 2
MESH = pl.DeviceIdType.MESH
VMEM_BYTES = 67_043_328


def fused_kernel(
    n_fs, n_tp,
    stream, w_up, w_down, w_in, w_out, pool_w, norm_gain, ffn_gain, s_in, s_out, s_up, s_down,
    out,
    up_all, down_all, up_other, down_other, ffn_rows, hidden, mixed, in_all, out_all,
    pool_in, grouped, squares, core_got, core_sent, pair_got, pair_sent, totals, pair_total,
    up_floats, own_scales, scales, scale_in, scale_out, scale_up,
    load_sem, scale_send, scale_recv,
    mix_recv, mix_own_send, mix_z_send, mix_x_send, mix_y_send,
    piece_recv, own_send, z_send, x_send, y_send,
    core_send, core_recv, act_core_send, act_core_recv, act_pair_send, act_pair_recv,
    part_core_send, part_core_recv, part_pair_send, part_pair_recv, store_sem,
):
    rep, fs, tp = lax.axis_index("rep"), lax.axis_index("fs"), lax.axis_index("tp")
    n_z = n_fs // 2
    z, y = fs // 2, fs % 2
    length, local = stream.shape
    width = n_tp * local
    units = up_all.shape[1]
    block = down_all.shape[2]
    owned = n_fs // n_tp
    in_rows, out_rows = w_in.shape[0], w_out.shape[0]
    pool_width = pool_in.shape[1]
    core, across, pair = {"tp": 1 - tp}, {"rep": 1 - rep}, {"fs": fs + 1 - 2 * y}

    def remote(ref, there, sent, got, device):
        return pltpu.make_async_remote_copy(
            src_ref=ref, dst_ref=there, send_sem=sent, recv_sem=got,
            device_id=device, device_id_type=MESH,
        )

    def at_step(i):
        j, other = i // 2, i % 2
        both = jnp.minimum(z, n_z - 1 - z)
        paired = j <= 2 * both
        distance = jnp.where(paired, (j + 1) // 2, j - both)
        left = jnp.where(paired, j % 2 == 1, z > n_z - 1 - z)
        source = z + jnp.where(left, -distance, distance)
        return source * 2 + y + other - 2 * y * other, left

    def onward(left):
        return jnp.where(left, z < n_z - 1, z > 0), {"fs": fs + jnp.where(left, 2, -2)}

    up_piece, down_piece = up_other.shape[0] // (2 * PARTS), units // (2 * PARTS)

    def piece(kind, source, half, q):
        place = half * PARTS + q
        if kind == 0:
            start = (source * 2 * PARTS + place) * up_piece
            return up_all.at[pl.ds(pl.multiple_of(start, up_piece), up_piece), :]
        return down_all.at[source, pl.ds(pl.multiple_of(place * down_piece, down_piece), down_piece), :]

    def mix_piece(kind, source, half):
        ref, rows = ((in_all, in_rows), (out_all, out_rows))[kind]
        return ref.at[pl.ds(pl.multiple_of(source * rows + half * (rows // 2), rows // 2), rows // 2), :]

    def own_copy(kind, order, side, q):
        source = fs if order == 0 else fs + 1 - 2 * y
        ref = piece(kind, source, rep, q)
        return remote(ref, ref, own_send.at[kind, side, order, q], piece_recv.at[kind, source, rep, q],
                      {"fs": fs + (2 if side == 0 else -2)})

    def pair_copy(kind, half, q):
        size = (up_piece, down_piece)[kind]
        ref = (up_other, down_other)[kind].at[pl.ds(pl.multiple_of((half * PARTS + q) * size, size), size), :]
        return remote(ref, piece(kind, fs, half, q), y_send.at[kind, half, q], piece_recv.at[kind, fs, half, q], pair)

    def onward_copy(kind, source, q, device):
        ref = piece(kind, source, rep, q)
        return remote(ref, ref, z_send.at[kind, source, q], piece_recv.at[kind, source, rep, q], device)

    def across_copy(kind, source, q):
        ref = piece(kind, source, rep, q)
        return remote(ref, ref, x_send.at[kind, source, q], piece_recv.at[kind, source, rep, q], across)

    def piece_wait(kind, source, half, q):
        ref = piece(kind, source, half, q)
        remote(ref, ref, x_send.at[kind, source, q], piece_recv.at[kind, source, half, q], across).wait_recv()

    def other_half(kind, source):
        for q in range(PARTS):
            piece_wait(kind, source, 1 - rep, q)

    def both_sides(act):
        @pl.when(z < n_z - 1)
        def _():
            act(0)

        @pl.when(z > 0)
        def _():
            act(1)

    def send_own(kind, q):
        both_sides(lambda side: own_copy(kind, 0, side, q).start())

    def send_pair(kind):
        for turn in range(2):
            for q in range(PARTS):
                pair_copy(kind, rep + turn - 2 * rep * turn, q).start()

    def pass_pair(kind):
        for q in range(PARTS):
            piece_wait(kind, fs + 1 - 2 * y, rep, q)
            both_sides(lambda side, q=q: own_copy(kind, 1, side, q).start())

    def pass_on(kind, i):
        source, left = at_step(i)
        going, device = onward(left)
        for q in range(PARTS):
            piece_wait(kind, source, rep, q)

            @pl.when(going)
            def _():
                onward_copy(kind, source, q, device).start()

            across_copy(kind, source, q).start()

    def mix_own_copy(kind, side):
        ref = mix_piece(kind, fs, rep)
        return remote(ref, ref, mix_own_send.at[kind, side], mix_recv.at[kind, fs, rep],
                      {"fs": fs + (2 if side == 0 else -2)})

    def mix_onward_copy(kind, source, device):
        ref = mix_piece(kind, source, rep)
        return remote(ref, ref, mix_z_send.at[kind, source], mix_recv.at[kind, source, rep], device)

    def mix_across_copy(kind, source):
        ref = mix_piece(kind, source, rep)
        return remote(ref, ref, mix_x_send.at[kind, source], mix_recv.at[kind, source, rep], across)

    def mix_pair_copy(kind, source, half):
        ref = mix_piece(kind, source, half)
        return remote(ref, ref, mix_y_send.at[kind, source, half], mix_recv.at[kind, source, half], pair)

    def mix_wait(kind, source, half):
        mix_pair_copy(kind, source, half).wait_recv()

    def scale_copy(offset):
        return remote(own_scales, scales.at[fs], scale_send.at[offset], scale_recv.at[fs],
                      {"fs": lax.rem(fs + offset, n_fs)})

    def core_copy(which, ref, there):
        return remote(ref, there, core_send.at[which], core_recv.at[which], core)

    my_half = pl.ds(pl.multiple_of(tp * local, local), local)
    my_pool = pl.ds(pl.multiple_of(tp * pool_width, pool_width), pool_width)
    n_tiles = 4
    tile = length // n_tiles

    def rows_of(t):
        return pl.ds(pl.multiple_of(t * tile, tile), tile)

    def act_pair_copy(t):
        return remote(ffn_rows.at[0, rows_of(t), my_half], ffn_rows.at[1, rows_of(t), my_half],
                      act_pair_send.at[t], act_pair_recv.at[t], pair)

    def act_core_copy(which, t):
        ref = ffn_rows.at[which, rows_of(t), my_half]
        return remote(ref, ref, act_core_send.at[which, t], act_core_recv.at[which, t], core)

    load_tokens = pltpu.make_async_copy(stream, mixed, load_sem.at[0])

    def load_up(which, half):
        return pltpu.make_async_copy(
            w_up.at[:, pl.ds(pl.multiple_of(half * units, units), units)], up_floats, load_sem.at[1 + which])

    quarter = units // 2

    def load_down(q):
        return pltpu.make_async_copy(
            w_down.at[pl.ds(q * quarter, quarter), :], totals.at[q], load_sem.at[3 + q])

    load_tokens.start()
    load_up(0, y).start()
    for q in range(4):
        load_down(q).start()

    own_in = pl.ds(pl.multiple_of(fs * in_rows, in_rows), in_rows)
    own_out = pl.ds(pl.multiple_of(fs * out_rows, out_rows), out_rows)
    in_all[own_in, :] = w_in[...].astype(bf16)
    out_all[own_out, :] = w_out[...].astype(bf16)

    up_lines, down_lines = s_up.shape[1] // LANES, block // LANES
    own_scales[0:1, 0:s_in.shape[1]] = s_in[...]
    own_scales[1:2, :] = s_out[...]
    for i in range(up_lines):
        own_scales[2 + i:3 + i, :] = s_up[:, i * LANES:(i + 1) * LANES]
    for i in range(down_lines):
        line = 2 + up_lines + i
        own_scales[line:line + 1, :] = s_down[:, i * LANES:(i + 1) * LANES]

    barrier = pltpu.get_barrier_semaphore()
    for offset in range(1, n_fs):
        pl.semaphore_signal(barrier, inc=1, device_id={"fs": lax.rem(fs + offset, n_fs)}, device_id_type=MESH)
    pl.semaphore_signal(barrier, inc=1, device_id=across, device_id_type=MESH)
    pl.semaphore_signal(barrier, inc=1, device_id=core, device_id_type=MESH)

    pieces = 8
    up_tile = up_floats.shape[0] // pieces

    def cast_own(t, carry):
        rows = pl.ds(pl.multiple_of(t * up_tile, up_tile), up_tile)
        there = pl.ds(pl.multiple_of(fs * up_floats.shape[0] + t * up_tile, up_tile), up_tile)
        up_all[there, :] = up_floats[rows, :].astype(bf16)
        return carry

    def cast_other(t, carry):
        rows = pl.ds(pl.multiple_of(t * up_tile, up_tile), up_tile)
        up_other[rows, :] = up_floats[rows, :].astype(bf16)
        return carry

    def square_rows(t, carry):
        floats = mixed[rows_of(t), :].astype(f32)
        total = jnp.sum(floats * floats, axis=1, keepdims=True)
        squares[0, rows_of(t), :] = jnp.broadcast_to(total, (tile, LANES))
        return carry

    load_up(0, y).wait()
    lax.fori_loop(0, pieces, cast_own, 0)
    load_up(1, 1 - y).start()
    load_tokens.wait()
    lax.fori_loop(0, n_tiles, square_rows, 0)
    pl.semaphore_wait(barrier, n_fs + 1)

    for kind in range(2):
        both_sides(lambda side, kind=kind: mix_own_copy(kind, side).start())
        for half in range(2):
            mix_pair_copy(kind, fs, half).start()
    for offset in range(1, n_fs):
        scale_copy(offset).start()
    share_squares = core_copy(0, squares.at[0], squares.at[1])
    share_squares.start()
    scales[fs] = own_scales[...]

    def mix_step(j):
        source, left = at_step(2 * j)
        going, device = onward(left)
        for kind in range(2):
            mix_wait(kind, source, rep)

            @pl.when(going)
            def _():
                mix_onward_copy(kind, source, device).start()

            mix_across_copy(kind, source).start()
            mix_pair_copy(kind, source, rep).start()

    load_up(1, 1 - y).wait()
    lax.fori_loop(0, pieces, cast_other, 0)
    share_squares.wait()

    def normed_rows(t, carry):
        rows = rows_of(t)
        total = squares[0, rows, :] + squares[1, rows, :]
        scale = lax.rsqrt(total[:, :1] * (1.0 / width) + epsilon)
        floats = mixed[rows, :].astype(f32)
        hidden[1, rows, my_half] = (floats * scale * norm_gain[:, my_half]).astype(bf16)
        return carry

    lax.fori_loop(0, n_tiles, normed_rows, 0)
    share_normed = core_copy(1, hidden.at[1, :, my_half], hidden.at[1, :, my_half])
    share_normed.start()

    for j in range(1, n_z):
        mix_step(j)
    for q in range(PARTS):
        send_own(0, q)

    for q in range(4):
        load_down(q).wait()
    down_tile = quarter // pieces

    def cast_down(t, carry):
        rows = pl.ds(pl.multiple_of(t * down_tile, down_tile), down_tile)
        for half in range(2):
            there = pl.ds(pl.multiple_of(half * quarter + t * down_tile, down_tile), down_tile)
            down_all[fs, there, :] = totals[2 * y + half, rows, :].astype(bf16)
            down_other[there, :] = totals[2 - 2 * y + half, rows, :].astype(bf16)
        return carry

    inner = jnp.minimum(z, n_z - 1 - z) > 0

    def inner_pass(kind, i):
        @pl.when(inner)
        def _():
            pass_on(kind, i)

    def outer_pass(kind, i):
        @pl.when(jnp.logical_not(inner))
        def _():
            pass_on(kind, i)

    for j in range(1, n_z):
        source, _ = at_step(2 * j)
        for kind in range(2):
            mix_wait(kind, source, 1 - rep)
            mix_pair_copy(kind, source, 1 - rep).start()
    send_pair(0)
    lax.fori_loop(0, pieces, cast_down, 0)
    for q in range(PARTS):
        send_own(1, q)
    pass_on(0, 2)
    inner_pass(0, 4)

    for offset in range(1, n_fs):
        source = lax.rem(fs + offset, n_fs)
        remote(own_scales, scales.at[source], scale_send.at[offset], scale_recv.at[source], pair).wait_recv()
    few = s_in.shape[1]
    for source in range(n_fs):
        scale_in[:, source * few:(source + 1) * few] = scales[source, 0:1, 0:few]
        scale_out[:, source * LANES:(source + 1) * LANES] = scales[source, 1:2, :]
    per = up_lines * LANES
    for q in range(n_fs // 2):
        rows = scales[y * (n_fs // 2) + q]
        for i in range(up_lines):
            scale_up[:, q * per + i * LANES:q * per + (i + 1) * LANES] = rows[2 + i:3 + i, :]

    for source_z in range(n_z):
        for kind in range(2):
            for half in range(2):
                mix_wait(kind, source_z * 2 + 1 - y, half)

    share_normed.wait()

    def pool_rows(t, carry):
        rows = rows_of(t)
        product = jnp.dot(hidden[1, rows, :], in_all[...], preferred_element_type=f32)
        pool_in[rows, :] = (product * scale_in[...]).astype(bf16)
        return carry

    lax.fori_loop(0, n_tiles, pool_rows, 0)
    per_core = pool_width // GROUP

    def group_rows(t, carry):
        rows = rows_of(t)
        target = lax.broadcasted_iota(jnp.int32, (tile, length), 0) + t * tile
        source = lax.broadcasted_iota(jnp.int32, (tile, length), 1)
        gap = source - target
        at = lax.broadcasted_iota(jnp.int32, (tile, GROUP), 0) + t * tile
        for g in range(per_core):
            half = jnp.left_shift(jnp.int32(1), tp * per_core + g)
            lanes = slice(g * GROUP, (g + 1) * GROUP)
            band = jnp.where((gap >= -half) & (gap < half), 1.0, 0.0).astype(bf16)
            sums = jnp.dot(band, pool_in[:, lanes], preferred_element_type=f32)
            counts = (jnp.minimum(at + half, length) - jnp.maximum(at - half, 0)).astype(f32)
            pooled = (sums / counts - pool_in[rows, lanes].astype(f32)).astype(bf16)
            product = jnp.dot(pooled, pool_w[tp * per_core + g], preferred_element_type=f32)
            there = pl.ds(pl.multiple_of(tp * pool_width + g * GROUP, GROUP), GROUP)
            grouped[rows, there] = product.astype(bf16)
        return carry

    lax.fori_loop(0, n_tiles, group_rows, 0)
    share_grouped = core_copy(2, grouped.at[:, my_pool], grouped.at[:, my_pool])
    share_grouped.start()
    outer_pass(1, 2)
    pass_pair(0)
    share_grouped.wait()

    def mix_rows(t, carry):
        rows = rows_of(t)
        product = jnp.dot(grouped[rows, :], out_all[...], preferred_element_type=f32)
        total = (mixed[rows, :].astype(f32) + product * scale_out[...]).astype(bf16)
        mixed[rows, :] = total
        floats = total.astype(f32)
        squares[0, rows, :] = jnp.broadcast_to(jnp.sum(floats * floats, axis=1, keepdims=True), (tile, LANES))
        return carry

    lax.fori_loop(0, n_tiles, mix_rows, 0)
    share_more = core_copy(3, squares.at[0], squares.at[1])
    share_more.start()
    inner_pass(0, 6)
    outer_pass(0, 4)
    share_more.wait()

    def ffn_in_rows(t, carry):
        rows = rows_of(t)
        total = squares[0, rows, :] + squares[1, rows, :]
        scale = lax.rsqrt(total[:, :1] * (1.0 / width) + epsilon)
        floats = mixed[rows, :].astype(f32)
        ffn_rows[0, rows, my_half] = (floats * scale * ffn_gain[:, my_half]).astype(bf16)
        act_pair_copy(t).start()
        act_core_copy(0, t).start()
        return carry

    lax.fori_loop(0, n_tiles, ffn_in_rows, 0)
    send_pair(1)

    pass_on(0, 3)
    outer_pass(0, 6)
    pass_on(0, 5)
    pass_on(0, 7)
    inner_pass(1, 2)
    inner_pass(1, 4)
    inner_pass(1, 6)
    other_half(0, fs + 1 - 2 * y)

    def up_ready(i, carry):
        source, _ = at_step(i)
        other_half(0, source)
        return carry

    lax.fori_loop(2, 2 * n_z, up_ready, 0)
    for t in range(n_tiles):
        act_core_copy(0, t).wait_recv()

    up_rows, up_columns = UP_TILE
    n_rows, n_columns = length // up_rows, units // up_columns
    half_tiles = n_rows * n_columns // 2

    def up_tiles(sequence):
        def body(n, carry):
            rows = pl.ds(pl.multiple_of((n % n_rows) * up_rows, up_rows), up_rows)
            columns = pl.ds(pl.multiple_of((n // n_rows) * up_columns, up_columns), up_columns)
            product = jnp.dot(ffn_rows[sequence, rows, :], up_all[:, columns], preferred_element_type=f32)
            positive = jnp.maximum(product * scale_up[:, columns], 0.0)
            hidden[sequence, rows, columns] = (positive * positive).astype(bf16)
            return carry

        return body

    for t in range(n_tiles):
        act_pair_copy(t).wait_recv()
        act_core_copy(1, t).start()
    lax.fori_loop(0, half_tiles, up_tiles(0), 0)
    outer_pass(1, 4)
    lax.fori_loop(half_tiles, 2 * half_tiles, up_tiles(0), 0)
    pass_pair(1)
    for t in range(n_tiles):
        act_core_copy(1, t).wait_recv()
    lax.fori_loop(0, half_tiles, up_tiles(1), 0)
    outer_pass(1, 6)
    lax.fori_loop(half_tiles, 2 * half_tiles, up_tiles(1), 0)

    down_rows, n_parts = DOWN_ROWS, length // DOWN_ROWS

    def part_core_copy(index, sequence, m):
        span = pl.ds(pl.multiple_of(sequence * length + m * down_rows, down_rows), down_rows)
        return remote(core_sent.at[index, span, :], core_got.at[index, span, :],
                      part_core_send.at[index, sequence, m], part_core_recv.at[index, sequence, m], core)

    def part_pair_copy(index, m):
        span = pl.ds(pl.multiple_of(m * down_rows, down_rows), down_rows)
        return remote(pair_sent.at[index, span, :], pair_got.at[index, span, :],
                      part_pair_send.at[index, m], part_pair_recv.at[index, m], pair)

    def down_order(n):
        return jnp.where(n < n_z, 2 * n, 2 * (n - n_z) + 1)

    def down_block(n, carry):
        @pl.when(inner & (n >= 1) & (n < n_z - 1))
        def _():
            pass_on(1, 2 * n + 1)

        @pl.when(jnp.logical_not(inner) & (n % 2 == 1) & (n < 2 * n_z - 4))
        def _():
            pass_on(1, n + 2)

        @pl.when(n == 2 * n_z - 3)
        def _():
            pass_on(1, 2 * n_z - 1)

        source, _ = at_step(down_order(n))

        @pl.when(n > 0)
        def _():
            other_half(1, source)

        index = source % owned
        mine = source // owned == tp
        lines = [2 + up_lines + i for i in range(down_lines)]
        scale = jnp.concatenate([scales[source, line:line + 1, :] for line in lines], axis=1)

        def part(sequence, m):
            rows = pl.ds(pl.multiple_of(m * down_rows, down_rows), down_rows)
            product = jnp.dot(hidden[sequence, rows, :], down_all[source], preferred_element_type=f32) * scale

            @pl.when(mine)
            def _():
                if sequence == 1:
                    pair_total[rows, :] = product
                else:
                    totals[index, rows, :] = product

            @pl.when(jnp.logical_not(mine))
            def _():
                core_sent[index, pl.ds(pl.multiple_of(sequence * length + m * down_rows, down_rows), down_rows), :] = product.astype(bf16)
                part_core_copy(index, sequence, m).start()

        def hand_over(m):
            @pl.when(mine)
            def _():
                rows = pl.ds(pl.multiple_of(m * down_rows, down_rows), down_rows)
                part_core_copy(index, 1, m).wait_recv()
                got = core_got[index, pl.ds(pl.multiple_of(length + m * down_rows, down_rows), down_rows), :].astype(f32)
                pair_sent[index, rows, :] = (pair_total[rows, :] + got).astype(bf16)
                part_pair_copy(index, m).start()

        def theirs(m, inner_carry):
            part(1, m)
            return inner_carry

        def ours(m, inner_carry):
            hand_over(m)
            part(0, m)
            return inner_carry

        lax.fori_loop(0, n_parts, theirs, 0)
        lax.fori_loop(0, n_parts, ours, 0)
        return carry

    lax.fori_loop(0, n_fs, down_block, 0)

    def store_block(index, m):
        rows = pl.ds(pl.multiple_of(m * down_rows, down_rows), down_rows)
        columns = pl.ds(pl.multiple_of(index * block, block), block)
        return pltpu.make_async_copy(pair_sent.at[index, rows, :], out.at[rows, columns], store_sem.at[index, m])

    def finish_block(i, carry):
        source, _ = at_step(down_order(i))

        @pl.when(source // owned == tp)
        def _():
            index = source % owned
            columns = pl.ds(pl.multiple_of(index * block, block), block)
            for m in range(n_parts):
                rows = pl.ds(pl.multiple_of(m * down_rows, down_rows), down_rows)
                part_core_copy(index, 0, m).wait_recv()
                part_pair_copy(index, m).wait()
                total = totals[index, rows, :] + core_got[index, rows, :].astype(f32)
                total = total + pair_got[index, rows, :].astype(f32)
                pair_sent[index, rows, :] = (mixed[rows, columns].astype(f32) + total).astype(bf16)
                store_block(index, m).start()

        return carry

    lax.fori_loop(0, n_fs, finish_block, 0)

    for kind in range(2):
        both_sides(lambda side, kind=kind: mix_own_copy(kind, side).wait_send())
        for q in range(PARTS):
            for order in range(2):
                both_sides(lambda side, kind=kind, order=order, q=q: own_copy(kind, order, side, q).wait_send())
            for half in range(2):
                pair_copy(kind, half, q).wait_send()
        for half in range(2):
            mix_pair_copy(kind, fs, half).wait_send()

        def sent_step(i, carry, kind=kind):
            source, left = at_step(i)
            going, device = onward(left)

            for q in range(PARTS):
                @pl.when(going)
                def _():
                    onward_copy(kind, source, q, device).wait_send()

                across_copy(kind, source, q).wait_send()

            @pl.when(i % 2 == 0)
            def _():
                @pl.when(going)
                def _():
                    mix_onward_copy(kind, source, device).wait_send()

                mix_across_copy(kind, source).wait_send()
                mix_pair_copy(kind, source, 0).wait_send()
                mix_pair_copy(kind, source, 1).wait_send()

            return carry

        lax.fori_loop(2, 2 * n_z, sent_step, 0)
    for offset in range(1, n_fs):
        scale_copy(offset).wait_send()
    for t in range(n_tiles):
        act_pair_copy(t).wait_send()
        for which in range(2):
            act_core_copy(which, t).wait_send()
    for index in range(owned):
        for m in range(n_parts):
            for sequence in range(2):
                part_core_copy(index, sequence, m).wait_send()
            store_block(index, m).wait()


def fused(n_fs, n_tp, stream, norm_gain, w_in, s_in, pool_w, w_out, s_out,
          ffn_gain, w_up, s_up, w_down, s_down):
    tokens = stream[0]
    length, local = tokens.shape
    rows, all_units = w_up.shape
    units = all_units // 2
    block = w_down.shape[1]
    in_rows, pool_width = w_in.shape
    out_rows = w_out.shape[0]
    owned = n_fs // n_tp
    parts = length // DOWN_ROWS
    lines = -(-(2 + (s_up.shape[0] + block) // LANES) // 8) * 8
    vmem, anywhere = pl.BlockSpec(memory_space=pltpu.VMEM), pl.BlockSpec(memory_space=pl.ANY)
    dma = pltpu.SemaphoreType.DMA
    result = pl.pallas_call(
        functools.partial(fused_kernel, n_fs, n_tp),
        out_shape=jax.ShapeDtypeStruct((length, local), bf16),
        in_specs=[anywhere] * 3 + [vmem] * 9,
        out_specs=anywhere,
        scratch_shapes=[
            pltpu.VMEM((rows * n_fs, units), bf16),
            pltpu.VMEM((n_fs, units, block), bf16),
            pltpu.VMEM((rows, units), bf16),
            pltpu.VMEM((units, block), bf16),
            pltpu.VMEM((2, length, n_tp * local), bf16),
            pltpu.VMEM((2, length, units), bf16),
            pltpu.VMEM((length, local), bf16),
            pltpu.VMEM((in_rows * n_fs, pool_width), bf16),
            pltpu.VMEM((out_rows * n_fs, local), bf16),
            pltpu.VMEM((length, pool_width), bf16),
            pltpu.VMEM((length, n_tp * pool_width), bf16),
            pltpu.VMEM((2, length, LANES), f32),
            pltpu.VMEM((owned, 2 * length, block), bf16),
            pltpu.VMEM((owned, 2 * length, block), bf16),
            pltpu.VMEM((owned, length, block), bf16),
            pltpu.VMEM((owned, length, block), bf16),
            pltpu.VMEM((owned, length, block), f32),
            pltpu.VMEM((length, block), f32),
            pltpu.VMEM((rows, units), f32),
            pltpu.VMEM((lines, LANES), f32),
            pltpu.VMEM((n_fs, lines, LANES), f32),
            pltpu.VMEM((1, pool_width), f32),
            pltpu.VMEM((1, local), f32),
            pltpu.VMEM((1, units), f32),
            dma((7,)), dma((n_fs,)), dma((n_fs,)),
            dma((2, n_fs, 2)), dma((2, 2)), dma((2, n_fs)), dma((2, n_fs)), dma((2, n_fs, 2)),
            dma((2, n_fs, 2, PARTS)), dma((2, 2, 2, PARTS)), dma((2, n_fs, PARTS)), dma((2, n_fs, PARTS)),
            dma((2, 2, PARTS)),
            dma((4,)), dma((4,)), dma((2, 4)), dma((2, 4)), dma((4,)), dma((4,)),
            dma((owned, 2, parts)), dma((owned, 2, parts)), dma((owned, parts)), dma((owned, parts)), dma((owned, parts)),
        ],
        compiler_params=pltpu.CompilerParams(
            collective_id=0, has_side_effects=True, vmem_limit_bytes=VMEM_BYTES
        ),
        name="fused_layer",
    )(tokens, w_up, w_down, w_in, w_out, pool_w,
      norm_gain[None], ffn_gain[None], s_in[None], s_out[None], s_up[None], s_down[None])
    return result[None]


def fits(n_rep, n_fs, n_tp, args):
    stream, w_in, pool_w, s_out, s_up, w_down = args[0], args[2], args[4], args[6], args[9], args[10]
    return (
        n_rep == 2 and n_tp == 2 and n_fs % 4 == 0
        and stream.shape[0] == 1
        and pool_w.shape[0] * GROUP == w_in.shape[1] * n_tp
        and stream.shape[2] * n_tp == w_down.shape[1] * n_fs
        and s_out.shape[0] == LANES and s_up.shape[0] % LANES == 0 and w_down.shape[1] % LANES == 0
    )


def solution(mesh):
    n_rep, n_fs, n_tp = (mesh.shape[name] for name in ("rep", "fs", "tp"))

    def body(*args):
        if fits(n_rep, n_fs, n_tp, args):
            return fused(n_fs, n_tp, *args)
        return on_device(n_rep, n_fs, n_tp, *args)

    return jax.shard_map(
        body,
        mesh=mesh,
        in_specs=(
            P(("rep", "fs"), None, "tp"),
            P(),
            P("fs", "tp"),
            P(("tp", "fs")),
            P(),
            P("fs", "tp"),
            P(("tp", "fs")),
            P(),
            P("fs", "tp"),
            P(("tp", "fs")),
            P("tp", "fs"),
            P("fs"),
        ),
        out_specs=P(("rep", "fs"), None, "tp"),
        check_vma=False,
    )
```

```python
import functools

import jax
import jax.numpy as jnp
from jax import lax
from jax.experimental import pallas as pl
from jax.experimental.pallas import tpu as pltpu
from jax.sharding import PartitionSpec as P

GROUP = 128


epsilon = 0.25
bf16 = jnp.bfloat16
f32 = jnp.float32


def dot(left, right):
    return jnp.dot(left, right, preferred_element_type=f32)


def rms_rows(values, gain):
    floats = values.astype(f32)
    scale = lax.rsqrt(jnp.mean(floats * floats, axis=-1, keepdims=True) + epsilon)
    return (floats * scale * gain).astype(bf16)


def shifted(value, axis_name, count, offset):
    return lax.ppermute(value, axis_name, [(i, (i + offset) % count) for i in range(count)])


def swap_gather(value, axis_name, count, axis):
    index = lax.axis_index(axis_name)
    width = value.shape[axis]
    shape = list(value.shape)
    shape[axis] = width * count
    if count == 2:
        other = shifted(value, axis_name, count, 1)
        low = jnp.where(index == 0, value, other)
        high = jnp.where(index == 0, other, value)
        return jnp.concatenate([low, high], axis=axis)
    full = jnp.zeros(shape, value.dtype)
    full = lax.dynamic_update_slice_in_dim(full, value, index * width, axis)
    for offset in range(1, count):
        piece = shifted(value, axis_name, count, offset)
        origin = (index - offset) % count
        full = lax.dynamic_update_slice_in_dim(full, piece, origin * width, axis)
    return full


def fs_sent(value, factors, offset_a, offset_b):
    n_a, n_b = factors
    pairs = []
    for i in range(n_a * n_b):
        pairs.append((i, ((i // n_b) ^ offset_a) * n_b + ((i % n_b) ^ offset_b)))
    return lax.ppermute(value, "fs", pairs)


def fs_pieces(value, factors):
    n_a, n_b = factors
    rows = [[value] for _ in range(n_a)]
    for x in range(1, n_a):
        rows[x] = [fs_sent(value, factors, x, 0)]
    for y in range(1, n_b):
        for x in range(n_a):
            rows[x].append(fs_sent(rows[x][0], factors, 0, y))
    return rows


def fs_origin(factors, x, y):
    index = lax.axis_index("fs")
    return ((index // factors[1]) ^ x) * factors[1] + ((index % factors[1]) ^ y)


def placed(rows, factors):
    block = rows[0][0].shape[0]
    width = rows[0][0].shape[1]
    full = jnp.zeros((block * factors[0] * factors[1], width), rows[0][0].dtype)
    for y in range(factors[1]):
        for x in range(factors[0]):
            full = lax.dynamic_update_slice_in_dim(
                full, rows[x][y], fs_origin(factors, x, y) * block, 0
            )
    return full


def pool_local(pool_in, first):
    length, width = pool_in.shape
    positions = jnp.arange(length, dtype=jnp.int32)
    source = positions[None, :]
    target = positions[:, None]
    group_of = (first + jnp.arange(width, dtype=jnp.int32)) // GROUP
    means = jnp.zeros((length, width), f32)
    for level in range(4):
        half = 2**level
        band_ones = ((source >= target - half) & (source < target + half)).astype(bf16)
        counts = (jnp.minimum(positions + half, length) - jnp.maximum(positions - half, 0)).astype(f32)
        sums = dot(band_ones, pool_in) / counts[:, None]
        means = jnp.where(group_of[None, :] == level, sums, means)
    return (means - pool_in.astype(f32)).astype(bf16)


def on_device(
    n_rep, n_fs, n_tp,
    stream, norm_gain, w_in, s_in, pool_w, w_out, s_out, ffn_gain, w_up, s_up, w_down, s_down,
):
    rep = lax.axis_index("rep")
    tokens = stream[0]
    length, local_width = tokens.shape
    hidden_width = w_up.shape[1] // n_rep

    n_a = n_tp * max(1, 4 // n_tp)
    factors = (n_a, n_fs // n_a)

    scales = jnp.concatenate([s_in, s_out, s_up, s_down])[None]
    scale_rows = [
        [scales if x == y == 0 else fs_sent(scales, factors, x, y) for y in range(factors[1])]
        for x in range(n_a)
    ]
    scales = placed(scale_rows, factors)
    ends, at = [], 0
    for part in (s_in, s_out, s_up, s_down):
        ends.append(scales[:, at:at + part.shape[0]])
        at += part.shape[0]
    scale_in, scale_out, scale_up = (part.reshape(-1) for part in ends[:3])
    scale_down = ends[3]

    in_rows = fs_pieces(w_in.astype(bf16), factors)
    out_rows = fs_pieces(w_out.astype(bf16), factors)
    w_in_all = placed(in_rows, factors)
    w_out_all = placed(out_rows, factors)

    up_own = lax.dynamic_slice_in_dim(w_up, rep * hidden_width, hidden_width, 1).astype(bf16)
    up_rows = fs_pieces(up_own, factors)
    up_all = placed(up_rows, factors)
    down_own = lax.dynamic_slice_in_dim(w_down, rep * hidden_width, hidden_width, 0).astype(bf16)
    down_own, *_ = lax.optimization_barrier((down_own, *[in_rows[x][0] for x in range(1, n_a)]))
    down_rows = fs_pieces(down_own, factors)

    normed = rms_rows(swap_gather(tokens, "tp", n_tp, 1), norm_gain)
    pool_in = (dot(normed, w_in_all) * scale_in).astype(bf16)
    pooled = pool_local(pool_in, lax.axis_index("tp") * pool_in.shape[1])
    pooled_all = swap_gather(pooled, "tp", n_tp, 1)
    groups = pool_w.shape[0]
    grouped = jnp.einsum(
        "lgc,gcd->lgd", pooled_all.reshape(length, groups, GROUP), pool_w, preferred_element_type=f32
    ).reshape(length, groups * GROUP).astype(bf16)
    mixed = (tokens.astype(f32) + dot(grouped, w_out_all) * scale_out).astype(bf16)

    mixed_own = swap_gather(mixed, "tp", n_tp, 1)
    sequences = [mixed_own]
    for offset in range(1, n_rep):
        other = shifted(mixed, "rep", n_rep, offset)
        sequences.append(swap_gather(other, "tp", n_tp, 1))
    scale_hidden = lax.dynamic_slice_in_dim(scale_up, rep * hidden_width, hidden_width, 0)
    hidden = []
    for rows in sequences:
        rows = rms_rows(rows, ffn_gain)
        upward = dot(rows, up_all)
        hidden.append(jnp.square(jax.nn.relu(upward * scale_hidden)).astype(bf16))

    hidden = jnp.concatenate(hidden, axis=0)
    width = w_down.shape[1]
    per_tp = n_a // n_tp
    tp = lax.axis_index("tp")
    turn = ((lax.axis_index("fs") // factors[1]) // per_tp) ^ tp
    result = jnp.zeros((length, local_width), bf16)
    for y in range(factors[1]):
        for xi in range(per_tp):
            stacked = jnp.stack([down_rows[xt * per_tp + xi][y] for xt in range(n_tp)])
            blocks, block_scales = [], []
            for k in range(n_tp):
                blocks.append(lax.dynamic_index_in_dim(stacked, turn ^ k, 0, keepdims=False))
                origin = fs_origin(factors, xi, y) ^ ((turn ^ k) * per_tp * factors[1])
                block_scales.append(lax.dynamic_index_in_dim(scale_down, origin, 0, keepdims=False))
            both = jnp.concatenate(blocks, axis=1)
            partial = (dot(hidden, both) * jnp.concatenate(block_scales)).astype(bf16)
            total = partial[:, :width].astype(f32)
            for k in range(1, n_tp):
                pairs = [(i, i ^ k) for i in range(n_tp)]
                total = total + lax.ppermute(partial[:, k * width:(k + 1) * width], "tp", pairs).astype(f32)
            own = total[:length]
            for k in range(1, n_rep):
                back = shifted(total[k * length:(k + 1) * length].astype(bf16), "rep", n_rep, -k)
                own = own + back.astype(f32)
            inner = (fs_origin(factors, xi, y) % (per_tp * factors[1])) * width
            mixed_part = lax.dynamic_slice_in_dim(mixed, inner, width, 1)
            piece = (mixed_part.astype(f32) + own).astype(bf16)
            result = lax.dynamic_update_slice_in_dim(result, piece, inner, 1)
    return result[None]


LANES = 128
UP_TILE = (512, 512)
DOWN_ROWS = 512
PARTS = 2
MESH = pl.DeviceIdType.MESH
VMEM_BYTES = 67_043_328


def fused_kernel(
    n_fs, n_tp,
    stream, w_up, w_down, w_in, w_out, pool_w, norm_gain, ffn_gain, s_in, s_out, s_up, s_down,
    out,
    up_all, down_all, up_other, down_other, ffn_rows, hidden, mixed, in_all, out_all,
    pool_in, grouped, squares, core_got, core_sent, pair_got, pair_sent, totals, pair_total,
    up_floats, own_scales, scales, scale_in, scale_out, scale_up,
    load_sem, scale_send, scale_recv,
    mix_recv, mix_own_send, mix_z_send, mix_x_send, mix_y_send,
    piece_recv, own_send, z_send, x_send, y_send,
    core_send, core_recv, act_core_send, act_core_recv, act_pair_send, act_pair_recv,
    part_core_send, part_core_recv, part_pair_send, part_pair_recv, store_sem,
):
    rep, fs, tp = lax.axis_index("rep"), lax.axis_index("fs"), lax.axis_index("tp")
    n_z = n_fs // 2
    z, y = fs // 2, fs % 2
    length, local = stream.shape
    width = n_tp * local
    units = up_all.shape[1]
    block = down_all.shape[2]
    owned = n_fs // n_tp
    in_rows, out_rows = w_in.shape[0], w_out.shape[0]
    pool_width = pool_in.shape[1]
    core, across, pair = {"tp": 1 - tp}, {"rep": 1 - rep}, {"fs": fs + 1 - 2 * y}

    def remote(ref, there, sent, got, device):
        return pltpu.make_async_remote_copy(
            src_ref=ref, dst_ref=there, send_sem=sent, recv_sem=got,
            device_id=device, device_id_type=MESH,
        )

    def at_step(i):
        j, other = i // 2, i % 2
        both = jnp.minimum(z, n_z - 1 - z)
        paired = j <= 2 * both
        distance = jnp.where(paired, (j + 1) // 2, j - both)
        left = jnp.where(paired, j % 2 == 1, z > n_z - 1 - z)
        source = z + jnp.where(left, -distance, distance)
        return source * 2 + y + other - 2 * y * other, left

    def onward(left):
        return jnp.where(left, z < n_z - 1, z > 0), {"fs": fs + jnp.where(left, 2, -2)}

    up_piece, down_piece = up_other.shape[0] // (2 * PARTS), units // (2 * PARTS)

    def piece(kind, source, half, q):
        place = half * PARTS + q
        if kind == 0:
            start = (source * 2 * PARTS + place) * up_piece
            return up_all.at[pl.ds(pl.multiple_of(start, up_piece), up_piece), :]
        return down_all.at[source, pl.ds(pl.multiple_of(place * down_piece, down_piece), down_piece), :]

    def mix_piece(kind, source, half):
        ref, rows = ((in_all, in_rows), (out_all, out_rows))[kind]
        return ref.at[pl.ds(pl.multiple_of(source * rows + half * (rows // 2), rows // 2), rows // 2), :]

    def own_copy(kind, order, side, q):
        source = fs if order == 0 else fs + 1 - 2 * y
        ref = piece(kind, source, rep, q)
        return remote(ref, ref, own_send.at[kind, side, order, q], piece_recv.at[kind, source, rep, q],
                      {"fs": fs + (2 if side == 0 else -2)})

    def pair_copy(kind, half, q):
        size = (up_piece, down_piece)[kind]
        ref = (up_other, down_other)[kind].at[pl.ds(pl.multiple_of((half * PARTS + q) * size, size), size), :]
        return remote(ref, piece(kind, fs, half, q), y_send.at[kind, half, q], piece_recv.at[kind, fs, half, q], pair)

    def onward_copy(kind, source, q, device):
        ref = piece(kind, source, rep, q)
        return remote(ref, ref, z_send.at[kind, source, q], piece_recv.at[kind, source, rep, q], device)

    def across_copy(kind, source, q):
        ref = piece(kind, source, rep, q)
        return remote(ref, ref, x_send.at[kind, source, q], piece_recv.at[kind, source, rep, q], across)

    def piece_wait(kind, source, half, q):
        ref = piece(kind, source, half, q)
        remote(ref, ref, x_send.at[kind, source, q], piece_recv.at[kind, source, half, q], across).wait_recv()

    def other_half(kind, source):
        for q in range(PARTS):
            piece_wait(kind, source, 1 - rep, q)

    def both_sides(act):
        @pl.when(z < n_z - 1)
        def _():
            act(0)

        @pl.when(z > 0)
        def _():
            act(1)

    def send_own(kind, q):
        both_sides(lambda side: own_copy(kind, 0, side, q).start())

    def send_pair(kind):
        for turn in range(2):
            for q in range(PARTS):
                pair_copy(kind, rep + turn - 2 * rep * turn, q).start()

    def pass_pair(kind):
        for q in range(PARTS):
            piece_wait(kind, fs + 1 - 2 * y, rep, q)
            both_sides(lambda side, q=q: own_copy(kind, 1, side, q).start())

    def pass_on(kind, i, parts=range(PARTS)):
        source, left = at_step(i)
        going, device = onward(left)
        for q in parts:
            piece_wait(kind, source, rep, q)

            @pl.when(going)
            def _():
                onward_copy(kind, source, q, device).start()

            across_copy(kind, source, q).start()

    def mix_own_copy(kind, side):
        ref = mix_piece(kind, fs, rep)
        return remote(ref, ref, mix_own_send.at[kind, side], mix_recv.at[kind, fs, rep],
                      {"fs": fs + (2 if side == 0 else -2)})

    def mix_onward_copy(kind, source, device):
        ref = mix_piece(kind, source, rep)
        return remote(ref, ref, mix_z_send.at[kind, source], mix_recv.at[kind, source, rep], device)

    def mix_across_copy(kind, source):
        ref = mix_piece(kind, source, rep)
        return remote(ref, ref, mix_x_send.at[kind, source], mix_recv.at[kind, source, rep], across)

    def mix_pair_copy(kind, source, half):
        ref = mix_piece(kind, source, half)
        return remote(ref, ref, mix_y_send.at[kind, source, half], mix_recv.at[kind, source, half], pair)

    def mix_wait(kind, source, half):
        mix_pair_copy(kind, source, half).wait_recv()

    def scale_copy(offset):
        return remote(own_scales, scales.at[fs], scale_send.at[offset], scale_recv.at[fs],
                      {"fs": lax.rem(fs + offset, n_fs)})

    def core_copy(which, ref, there):
        return remote(ref, there, core_send.at[which], core_recv.at[which], core)

    my_half = pl.ds(pl.multiple_of(tp * local, local), local)
    my_pool = pl.ds(pl.multiple_of(tp * pool_width, pool_width), pool_width)
    n_tiles = 4
    tile = length // n_tiles

    def rows_of(t):
        return pl.ds(pl.multiple_of(t * tile, tile), tile)

    def act_pair_copy(t):
        return remote(ffn_rows.at[0, rows_of(t), my_half], ffn_rows.at[1, rows_of(t), my_half],
                      act_pair_send.at[t], act_pair_recv.at[t], pair)

    def act_core_copy(which, t):
        ref = ffn_rows.at[which, rows_of(t), my_half]
        return remote(ref, ref, act_core_send.at[which, t], act_core_recv.at[which, t], core)

    load_tokens = pltpu.make_async_copy(stream, mixed, load_sem.at[0])

    def load_up(which, half):
        return pltpu.make_async_copy(
            w_up.at[:, pl.ds(pl.multiple_of(half * units, units), units)], up_floats, load_sem.at[1 + which])

    quarter = units // 2

    def load_down(q):
        return pltpu.make_async_copy(
            w_down.at[pl.ds(q * quarter, quarter), :], totals.at[q], load_sem.at[3 + q])

    load_tokens.start()
    load_up(0, y).start()
    for q in range(4):
        load_down(q).start()

    own_in = pl.ds(pl.multiple_of(fs * in_rows, in_rows), in_rows)
    own_out = pl.ds(pl.multiple_of(fs * out_rows, out_rows), out_rows)
    in_all[own_in, :] = w_in[...].astype(bf16)
    out_all[own_out, :] = w_out[...].astype(bf16)

    up_lines, down_lines = s_up.shape[1] // LANES, block // LANES
    own_scales[0:1, 0:s_in.shape[1]] = s_in[...]
    own_scales[1:2, :] = s_out[...]
    for i in range(up_lines):
        own_scales[2 + i:3 + i, :] = s_up[:, i * LANES:(i + 1) * LANES]
    for i in range(down_lines):
        line = 2 + up_lines + i
        own_scales[line:line + 1, :] = s_down[:, i * LANES:(i + 1) * LANES]

    barrier = pltpu.get_barrier_semaphore()
    for offset in range(1, n_fs):
        pl.semaphore_signal(barrier, inc=1, device_id={"fs": lax.rem(fs + offset, n_fs)}, device_id_type=MESH)
    pl.semaphore_signal(barrier, inc=1, device_id=across, device_id_type=MESH)
    pl.semaphore_signal(barrier, inc=1, device_id=core, device_id_type=MESH)

    pieces = 8
    up_tile = up_floats.shape[0] // pieces

    def cast_own(t, carry):
        rows = pl.ds(pl.multiple_of(t * up_tile, up_tile), up_tile)
        there = pl.ds(pl.multiple_of(fs * up_floats.shape[0] + t * up_tile, up_tile), up_tile)
        up_all[there, :] = up_floats[rows, :].astype(bf16)
        return carry

    def cast_other(t, carry):
        rows = pl.ds(pl.multiple_of(t * up_tile, up_tile), up_tile)
        up_other[rows, :] = up_floats[rows, :].astype(bf16)
        return carry

    def square_rows(t, carry):
        floats = mixed[rows_of(t), :].astype(f32)
        total = jnp.sum(floats * floats, axis=1, keepdims=True)
        squares[0, rows_of(t), :] = jnp.broadcast_to(total, (tile, LANES))
        return carry

    load_up(0, y).wait()
    lax.fori_loop(0, pieces, cast_own, 0)
    load_up(1, 1 - y).start()
    load_tokens.wait()
    lax.fori_loop(0, n_tiles, square_rows, 0)
    pl.semaphore_wait(barrier, n_fs + 1)

    for kind in range(2):
        both_sides(lambda side, kind=kind: mix_own_copy(kind, side).start())
        for half in range(2):
            mix_pair_copy(kind, fs, half).start()
    for offset in range(1, n_fs):
        scale_copy(offset).start()
    share_squares = core_copy(0, squares.at[0], squares.at[1])
    share_squares.start()
    scales[fs] = own_scales[...]

    def mix_step(j):
        source, left = at_step(2 * j)
        going, device = onward(left)
        for kind in range(2):
            mix_wait(kind, source, rep)

            @pl.when(going)
            def _():
                mix_onward_copy(kind, source, device).start()

            mix_across_copy(kind, source).start()
            mix_pair_copy(kind, source, rep).start()

    load_up(1, 1 - y).wait()
    lax.fori_loop(0, pieces, cast_other, 0)
    share_squares.wait()

    def normed_rows(t, carry):
        rows = rows_of(t)
        total = squares[0, rows, :] + squares[1, rows, :]
        scale = lax.rsqrt(total[:, :1] * (1.0 / width) + epsilon)
        floats = mixed[rows, :].astype(f32)
        hidden[1, rows, my_half] = (floats * scale * norm_gain[:, my_half]).astype(bf16)
        return carry

    lax.fori_loop(0, n_tiles, normed_rows, 0)
    share_normed = core_copy(1, hidden.at[1, :, my_half], hidden.at[1, :, my_half])
    share_normed.start()

    for j in range(1, n_z):
        mix_step(j)
    for q in range(PARTS):
        send_own(0, q)

    for q in range(4):
        load_down(q).wait()
    down_tile = quarter // pieces

    def cast_down(t, carry):
        rows = pl.ds(pl.multiple_of(t * down_tile, down_tile), down_tile)
        for half in range(2):
            there = pl.ds(pl.multiple_of(half * quarter + t * down_tile, down_tile), down_tile)
            down_all[fs, there, :] = totals[2 * y + half, rows, :].astype(bf16)
            down_other[there, :] = totals[2 - 2 * y + half, rows, :].astype(bf16)
        return carry

    inner = jnp.minimum(z, n_z - 1 - z) > 0

    def inner_pass(kind, i):
        @pl.when(inner)
        def _():
            pass_on(kind, i)

    def outer_pass(kind, i, parts=range(PARTS)):
        @pl.when(jnp.logical_not(inner))
        def _():
            pass_on(kind, i, parts)

    for j in range(1, n_z):
        source, _ = at_step(2 * j)
        for kind in range(2):
            mix_wait(kind, source, 1 - rep)
            mix_pair_copy(kind, source, 1 - rep).start()
    send_pair(0)
    lax.fori_loop(0, pieces, cast_down, 0)
    for q in range(PARTS):
        send_own(1, q)
    pass_on(0, 2)
    inner_pass(0, 4)

    for offset in range(1, n_fs):
        source = lax.rem(fs + offset, n_fs)
        remote(own_scales, scales.at[source], scale_send.at[offset], scale_recv.at[source], pair).wait_recv()
    few = s_in.shape[1]
    for source in range(n_fs):
        scale_in[:, source * few:(source + 1) * few] = scales[source, 0:1, 0:few]
        scale_out[:, source * LANES:(source + 1) * LANES] = scales[source, 1:2, :]
    per = up_lines * LANES
    for q in range(n_fs // 2):
        rows = scales[y * (n_fs // 2) + q]
        for i in range(up_lines):
            scale_up[:, q * per + i * LANES:q * per + (i + 1) * LANES] = rows[2 + i:3 + i, :]

    for source_z in range(n_z):
        for kind in range(2):
            for half in range(2):
                mix_wait(kind, source_z * 2 + 1 - y, half)

    share_normed.wait()

    def pool_rows(t, carry):
        rows = rows_of(t)
        product = jnp.dot(hidden[1, rows, :], in_all[...], preferred_element_type=f32)
        pool_in[rows, :] = (product * scale_in[...]).astype(bf16)
        return carry

    lax.fori_loop(0, n_tiles, pool_rows, 0)
    per_core = pool_width // GROUP

    def group_rows(t, carry):
        rows = rows_of(t)
        target = lax.broadcasted_iota(jnp.int32, (tile, length), 0) + t * tile
        source = lax.broadcasted_iota(jnp.int32, (tile, length), 1)
        gap = source - target
        at = lax.broadcasted_iota(jnp.int32, (tile, GROUP), 0) + t * tile
        for g in range(per_core):
            half = jnp.left_shift(jnp.int32(1), tp * per_core + g)
            lanes = slice(g * GROUP, (g + 1) * GROUP)
            band = jnp.where((gap >= -half) & (gap < half), 1.0, 0.0).astype(bf16)
            sums = jnp.dot(band, pool_in[:, lanes], preferred_element_type=f32)
            counts = (jnp.minimum(at + half, length) - jnp.maximum(at - half, 0)).astype(f32)
            pooled = (sums / counts - pool_in[rows, lanes].astype(f32)).astype(bf16)
            product = jnp.dot(pooled, pool_w[tp * per_core + g], preferred_element_type=f32)
            there = pl.ds(pl.multiple_of(tp * pool_width + g * GROUP, GROUP), GROUP)
            grouped[rows, there] = product.astype(bf16)
        return carry

    lax.fori_loop(0, n_tiles, group_rows, 0)
    share_grouped = core_copy(2, grouped.at[:, my_pool], grouped.at[:, my_pool])
    share_grouped.start()
    outer_pass(1, 2)
    pass_pair(0)
    share_grouped.wait()

    def mix_rows(t, carry):
        rows = rows_of(t)
        product = jnp.dot(grouped[rows, :], out_all[...], preferred_element_type=f32)
        total = (mixed[rows, :].astype(f32) + product * scale_out[...]).astype(bf16)
        mixed[rows, :] = total
        floats = total.astype(f32)
        squares[0, rows, :] = jnp.broadcast_to(jnp.sum(floats * floats, axis=1, keepdims=True), (tile, LANES))
        return carry

    lax.fori_loop(0, n_tiles, mix_rows, 0)
    share_more = core_copy(3, squares.at[0], squares.at[1])
    share_more.start()
    inner_pass(0, 6)
    outer_pass(0, 4)
    share_more.wait()

    def ffn_in_rows(t, carry):
        rows = rows_of(t)
        total = squares[0, rows, :] + squares[1, rows, :]
        scale = lax.rsqrt(total[:, :1] * (1.0 / width) + epsilon)
        floats = mixed[rows, :].astype(f32)
        ffn_rows[0, rows, my_half] = (floats * scale * ffn_gain[:, my_half]).astype(bf16)
        act_pair_copy(t).start()
        act_core_copy(0, t).start()
        return carry

    lax.fori_loop(0, n_tiles, ffn_in_rows, 0)
    send_pair(1)

    pass_on(0, 3)
    outer_pass(0, 6)
    pass_on(0, 5)
    pass_on(0, 7)
    inner_pass(1, 2)
    inner_pass(1, 4)
    inner_pass(1, 6)
    for t in range(n_tiles):
        act_pair_copy(t).wait_recv()
        act_core_copy(1, t).start()
    other_half(0, fs + 1 - 2 * y)

    def up_ready(i, carry):
        source, _ = at_step(i)
        other_half(0, source)
        return carry

    lax.fori_loop(2, 2 * n_z, up_ready, 0)
    for t in range(n_tiles):
        act_core_copy(0, t).wait_recv()

    up_rows, up_columns = UP_TILE
    n_rows, n_columns = length // up_rows, units // up_columns
    half_tiles = n_rows * n_columns // 2

    def up_tiles(sequence):
        def body(n, carry):
            rows = pl.ds(pl.multiple_of((n % n_rows) * up_rows, up_rows), up_rows)
            columns = pl.ds(pl.multiple_of((n // n_rows) * up_columns, up_columns), up_columns)
            product = jnp.dot(ffn_rows[sequence, rows, :], up_all[:, columns], preferred_element_type=f32)
            positive = jnp.maximum(product * scale_up[:, columns], 0.0)
            hidden[sequence, rows, columns] = (positive * positive).astype(bf16)
            return carry

        return body

    down_rows, n_parts = DOWN_ROWS, length // DOWN_ROWS

    def part_core_copy(index, sequence, m):
        span = pl.ds(pl.multiple_of(sequence * length + m * down_rows, down_rows), down_rows)
        return remote(core_sent.at[index, span, :], core_got.at[index, span, :],
                      part_core_send.at[index, sequence, m], part_core_recv.at[index, sequence, m], core)

    def part_pair_copy(index, m):
        span = pl.ds(pl.multiple_of(m * down_rows, down_rows), down_rows)
        return remote(pair_sent.at[index, span, :], pair_got.at[index, span, :],
                      part_pair_send.at[index, m], part_pair_recv.at[index, m], pair)

    def down_order(n):
        return jnp.where(n < n_z, 2 * n, 2 * (n - n_z) + 1)

    def block_of(n):
        source, _ = at_step(down_order(n))
        return source, source % owned, source // owned == tp

    def part(n, sequence, m):
        source, index, mine = block_of(n)
        lines = [2 + up_lines + i for i in range(down_lines)]
        scale = jnp.concatenate([scales[source, line:line + 1, :] for line in lines], axis=1)
        rows = pl.ds(pl.multiple_of(m * down_rows, down_rows), down_rows)
        product = jnp.dot(hidden[sequence, rows, :], down_all[source], preferred_element_type=f32) * scale

        @pl.when(mine)
        def _():
            if sequence == 1:
                pair_total[rows, :] = product
            else:
                totals[index, rows, :] = product

        @pl.when(jnp.logical_not(mine))
        def _():
            start = pl.multiple_of(sequence * length + m * down_rows, down_rows)
            core_sent[index, pl.ds(start, down_rows), :] = product.astype(bf16)
            part_core_copy(index, sequence, m).start()

    def hand_part(n, m):
        _, index, mine = block_of(n)

        @pl.when(mine)
        def _():
            rows = pl.ds(pl.multiple_of(m * down_rows, down_rows), down_rows)
            part_core_copy(index, 1, m).wait_recv()
            got = core_got[index, pl.ds(pl.multiple_of(length + m * down_rows, down_rows), down_rows), :].astype(f32)
            pair_sent[index, rows, :] = (pair_total[rows, :] + got).astype(bf16)
            part_pair_copy(index, m).start()

    def theirs(n):
        def body(m, carry):
            part(n, 1, m)
            return carry

        lax.fori_loop(0, n_parts, body, 0)

    def hand_over(n):
        def body(m, carry):
            hand_part(n, m)
            return carry

        lax.fori_loop(0, n_parts, body, 0)

    outer_pass(1, 4, range(1))
    for t in range(n_tiles):
        act_core_copy(1, t).wait_recv()
    lax.fori_loop(0, 3, up_tiles(1), 0)
    outer_pass(1, 4, range(1, PARTS))
    lax.fori_loop(3, 2 * half_tiles, up_tiles(1), 0)
    outer_pass(1, 6, range(1))
    theirs(0)
    pass_pair(1)
    lax.fori_loop(0, half_tiles, up_tiles(0), 0)
    hand_over(0)
    other_half(1, at_step(down_order(1))[0])
    theirs(1)
    outer_pass(1, 6, range(1, PARTS))
    lax.fori_loop(half_tiles, 2 * half_tiles, up_tiles(0), 0)
    hand_over(1)

    def sent_first():
        for kind in range(2):
            both_sides(lambda side, kind=kind: mix_own_copy(kind, side).wait_send())
            for q in range(PARTS):
                for order in range(2):
                    both_sides(lambda side, kind=kind, order=order, q=q: own_copy(kind, order, side, q).wait_send())
                for half in range(2):
                    pair_copy(kind, half, q).wait_send()
            for half in range(2):
                mix_pair_copy(kind, fs, half).wait_send()

        def sent_step(i, carry):
            source, left = at_step(i)
            going, device = onward(left)
            for q in range(PARTS):
                @pl.when(going)
                def _():
                    onward_copy(0, source, q, device).wait_send()

                across_copy(0, source, q).wait_send()

            @pl.when(i % 2 == 0)
            def _():
                for kind in range(2):
                    @pl.when(going)
                    def _():
                        mix_onward_copy(kind, source, device).wait_send()

                    mix_across_copy(kind, source).wait_send()
                    mix_pair_copy(kind, source, 0).wait_send()
                    mix_pair_copy(kind, source, 1).wait_send()

            return carry

        lax.fori_loop(2, 2 * n_z, sent_step, 0)
        for offset in range(1, n_fs):
            scale_copy(offset).wait_send()
        for t in range(n_tiles):
            act_pair_copy(t).wait_send()
            for which in range(2):
                act_core_copy(which, t).wait_send()

    def down_block(n, carry):
        @pl.when(inner & (n >= 1) & (n < n_z - 1))
        def _():
            pass_on(1, 2 * n + 1)

        @pl.when(jnp.logical_not(inner) & (n % 2 == 1) & (n >= 3) & (n < 2 * n_z - 2))
        def _():
            pass_on(1, n + 2, range(1, PARTS))

        @pl.when(inner & (n == 2 * n_z - 3))
        def _():
            pass_on(1, 2 * n_z - 1)

        source, _ = at_step(down_order(n))

        @pl.when(n == 2 * n_z - 1)
        def _():
            sent_first()

        @pl.when(n > 1)
        def _():
            other_half(1, source)

        @pl.when(n > 1)
        def _():
            theirs(n)

        @pl.when(jnp.logical_not(inner) & (n % 2 == 0) & (n < 2 * n_z - 3))
        def _():
            pass_on(1, n + 3, range(1))

        @pl.when(jnp.logical_not(inner) & (n == 1))
        def _():
            pass_on(1, 3, range(1, PARTS))

        def ours(m, inner_carry):
            @pl.when(n > 1)
            def _():
                hand_part(n, m)

            part(n, 0, m)
            return inner_carry

        lax.fori_loop(0, n_parts, ours, 0)
        return carry

    lax.fori_loop(0, n_fs, down_block, 0)

    def store_block(index, m):
        rows = pl.ds(pl.multiple_of(m * down_rows, down_rows), down_rows)
        columns = pl.ds(pl.multiple_of(index * block, block), block)
        return pltpu.make_async_copy(pair_sent.at[index, rows, :], out.at[rows, columns], store_sem.at[index, m])

    def finish_block(i, carry):
        source, _ = at_step(down_order(i))

        @pl.when(source // owned == tp)
        def _():
            index = source % owned
            columns = pl.ds(pl.multiple_of(index * block, block), block)
            for m in range(n_parts):
                rows = pl.ds(pl.multiple_of(m * down_rows, down_rows), down_rows)
                part_core_copy(index, 0, m).wait_recv()
                part_pair_copy(index, m).wait()
                total = totals[index, rows, :] + core_got[index, rows, :].astype(f32)
                total = total + pair_got[index, rows, :].astype(f32)
                pair_sent[index, rows, :] = (mixed[rows, columns].astype(f32) + total).astype(bf16)
                store_block(index, m).start()

        return carry

    lax.fori_loop(0, n_fs, finish_block, 0)

    def sent_last(i, carry):
        source, left = at_step(i)
        going, device = onward(left)
        for q in range(PARTS):
            @pl.when(going)
            def _():
                onward_copy(1, source, q, device).wait_send()

            across_copy(1, source, q).wait_send()

        return carry

    lax.fori_loop(2, 2 * n_z, sent_last, 0)
    for index in range(owned):
        for m in range(n_parts):
            for sequence in range(2):
                part_core_copy(index, sequence, m).wait_send()
            store_block(index, m).wait()


def fused(n_fs, n_tp, stream, norm_gain, w_in, s_in, pool_w, w_out, s_out,
          ffn_gain, w_up, s_up, w_down, s_down):
    tokens = stream[0]
    length, local = tokens.shape
    rows, all_units = w_up.shape
    units = all_units // 2
    block = w_down.shape[1]
    in_rows, pool_width = w_in.shape
    out_rows = w_out.shape[0]
    owned = n_fs // n_tp
    parts = length // DOWN_ROWS
    lines = -(-(2 + (s_up.shape[0] + block) // LANES) // 8) * 8
    vmem, anywhere = pl.BlockSpec(memory_space=pltpu.VMEM), pl.BlockSpec(memory_space=pl.ANY)
    dma = pltpu.SemaphoreType.DMA
    result = pl.pallas_call(
        functools.partial(fused_kernel, n_fs, n_tp),
        out_shape=jax.ShapeDtypeStruct((length, local), bf16),
        in_specs=[anywhere] * 3 + [vmem] * 9,
        out_specs=anywhere,
        scratch_shapes=[
            pltpu.VMEM((rows * n_fs, units), bf16),
            pltpu.VMEM((n_fs, units, block), bf16),
            pltpu.VMEM((rows, units), bf16),
            pltpu.VMEM((units, block), bf16),
            pltpu.VMEM((2, length, n_tp * local), bf16),
            pltpu.VMEM((2, length, units), bf16),
            pltpu.VMEM((length, local), bf16),
            pltpu.VMEM((in_rows * n_fs, pool_width), bf16),
            pltpu.VMEM((out_rows * n_fs, local), bf16),
            pltpu.VMEM((length, pool_width), bf16),
            pltpu.VMEM((length, n_tp * pool_width), bf16),
            pltpu.VMEM((2, length, LANES), f32),
            pltpu.VMEM((owned, 2 * length, block), bf16),
            pltpu.VMEM((owned, 2 * length, block), bf16),
            pltpu.VMEM((owned, length, block), bf16),
            pltpu.VMEM((owned, length, block), bf16),
            pltpu.VMEM((owned, length, block), f32),
            pltpu.VMEM((length, block), f32),
            pltpu.VMEM((rows, units), f32),
            pltpu.VMEM((lines, LANES), f32),
            pltpu.VMEM((n_fs, lines, LANES), f32),
            pltpu.VMEM((1, pool_width), f32),
            pltpu.VMEM((1, local), f32),
            pltpu.VMEM((1, units), f32),
            dma((7,)), dma((n_fs,)), dma((n_fs,)),
            dma((2, n_fs, 2)), dma((2, 2)), dma((2, n_fs)), dma((2, n_fs)), dma((2, n_fs, 2)),
            dma((2, n_fs, 2, PARTS)), dma((2, 2, 2, PARTS)), dma((2, n_fs, PARTS)), dma((2, n_fs, PARTS)),
            dma((2, 2, PARTS)),
            dma((4,)), dma((4,)), dma((2, 4)), dma((2, 4)), dma((4,)), dma((4,)),
            dma((owned, 2, parts)), dma((owned, 2, parts)), dma((owned, parts)), dma((owned, parts)), dma((owned, parts)),
        ],
        compiler_params=pltpu.CompilerParams(
            collective_id=0, has_side_effects=True, vmem_limit_bytes=VMEM_BYTES
        ),
        name="fused_layer",
    )(tokens, w_up, w_down, w_in, w_out, pool_w,
      norm_gain[None], ffn_gain[None], s_in[None], s_out[None], s_up[None], s_down[None])
    return result[None]


def fits(n_rep, n_fs, n_tp, args):
    stream, w_in, pool_w, s_out, s_up, w_down = args[0], args[2], args[4], args[6], args[9], args[10]
    return (
        n_rep == 2 and n_tp == 2 and n_fs % 4 == 0
        and stream.shape[0] == 1
        and pool_w.shape[0] * GROUP == w_in.shape[1] * n_tp
        and stream.shape[2] * n_tp == w_down.shape[1] * n_fs
        and s_out.shape[0] == LANES and s_up.shape[0] % LANES == 0 and w_down.shape[1] % LANES == 0
    )


def solution(mesh):
    n_rep, n_fs, n_tp = (mesh.shape[name] for name in ("rep", "fs", "tp"))

    def body(*args):
        if fits(n_rep, n_fs, n_tp, args):
            return fused(n_fs, n_tp, *args)
        return on_device(n_rep, n_fs, n_tp, *args)

    return jax.shard_map(
        body,
        mesh=mesh,
        in_specs=(
            P(("rep", "fs"), None, "tp"),
            P(),
            P("fs", "tp"),
            P(("tp", "fs")),
            P(),
            P("fs", "tp"),
            P(("tp", "fs")),
            P(),
            P("fs", "tp"),
            P(("tp", "fs")),
            P("tp", "fs"),
            P("fs"),
        ),
        out_specs=P(("rep", "fs"), None, "tp"),
        check_vma=False,
    )
```
